512 devices in a mesh: sp: 64 (over z, y), tp: 8 (over x, core).
Axes of the slice: x: 4, y: 8, z: 8, core: 2. Of those that a mesh axis runs over, the one named last changes fastest.
Arguments:
- tokens: bfloat16 [8192, 4096], P('sp'), may hold values from -6 to 6
- norm_gain: float32 [4096], replicated, may hold values from 0.1 to 1.9
- w_query: bfloat16 [4096, 2048], P('sp', 'tp'), may hold values from -1 to 1
- w_key: bfloat16 [4096, 512], P('sp', 'tp'), may hold values from -1 to 1
- w_value: bfloat16 [4096, 512], P('sp', 'tp'), may hold values from -0.09375 to 0.09375
- w_state_in: bfloat16 [4096, 2048], P('sp', 'tp'), may hold values from -0.09375 to 0.09375
- sink_logit: float32 [32], P('tp'), may hold values from 2 to 6
- decay_rate: float32 [128, 64], P('tp'), may hold values from 0.0002 to 4
- rotation: float32 [128, 64], P('tp'), may hold values from 1 to 60
- log_step: float32 [128], P('tp'), may hold values from -5.3 to -3
- in_re: float32 [128, 64, 16], P('tp'), may hold values from -1.5 to 1.5
- in_im: float32 [128, 64, 16], P('tp'), may hold values from -1.5 to 1.5
- out_re: float32 [128, 16, 64], P('tp'), may hold values from -0.75 to 0.75
- out_im: float32 [128, 16, 64], P('tp'), may hold values from -0.75 to 0.75
- skip_gain: float32 [2048], P('tp'), may hold values from -4 to 4
- w_attn_out: bfloat16 [2048, 4096], P('tp', 'sp'), may hold values from -0.5 to 0.5
- w_state_out: bfloat16 [2048, 4096], P('tp', 'sp'), may hold values from -0.125 to 0.125
- out_gain: float32 [4096], replicated, may hold values from 0.1 to 1.9
Outputs:
- mixed: bfloat16 [8192, 4096], P(('sp', 'tp'))
The draws below stay inside these ranges and needn't reach their ends.
All inputs are finite; a program needn't handle non-finite values.
Results may differ from the reference program's by a relative error of at most 0.015.
The reference program's roundings to bfloat16 on the way count: a program that leaves them out, or rounds other values in their place, can miss the bound.
Values may be sent and summed in bfloat16 or wider, within the bound.
A program may use at most 64 MiB of HBM per device.

```python
import math
import jax
import jax.numpy as jnp
from jax import lax

D = 4096
QH = 32
KVH = 8
HEAD = 64
GSIZE = 16
STATE = 64
WINDOW = 128
TOK_DEV = 128
ATTN = 2048
GROUPS = 128
TOKENS = 8192
N_SP = 64
N_TP = 8


def spiked_columns(key, salt, column_count):
    noise_part = jax.random.normal(jax.random.fold_in(key, salt), (D, column_count), jnp.float32) * D ** (-0.5)
    noise_part = jnp.clip(noise_part, -6.0 * D ** (-0.5), 6.0 * D ** (-0.5))
    return jnp.clip(noise_part, -1.0, 1.0)


def draw_w_query(key, part):
    return spiked_columns(key, 1, QH * HEAD).astype(jnp.bfloat16)


def draw_w_key(key, part):
    return spiked_columns(key, 2, KVH * HEAD).astype(jnp.bfloat16)


def draw_decay_rate(key, part):
    slow_rate = jnp.exp(jax.random.uniform(jax.random.fold_in(key, 11), (GROUPS, STATE), jnp.float32, math.log(0.0002), math.log(0.002)))
    fast_rate = jnp.exp(jax.random.uniform(jax.random.fold_in(key, 12), (GROUPS, STATE), jnp.float32, math.log(2.0), math.log(4.0)))
    picks = jax.random.randint(jax.random.fold_in(key, 13), (GROUPS, 1), 0, 10)
    slow_flag = picks < 5
    return jnp.where(slow_flag, slow_rate, fast_rate)


def levels(key, shape, pieces, smallest, top_value):
    gain = 1.0
    for axis_at, shards_of in pieces:
        heights = jax.random.uniform(jax.random.fold_in(jax.random.fold_in(key, 6), axis_at), (shards_of,), jnp.float32, smallest / len(pieces), top_value / len(pieces))
        gain = gain * jnp.repeat(jnp.exp(heights), shape[axis_at] // shards_of).reshape((-1,) + (1,) * (len(shape) - 1 - axis_at))
    return gain


def noise(key, dims, spread, bound, pieces=(), held_as=jnp.bfloat16):
    values = jax.random.normal(key, dims, jnp.float32) * spread
    if len(pieces) > 0:
        values = levels(key, dims, pieces, -0.22, 0.18) * values
    return jnp.clip(values, min=-bound, max=bound).astype(held_as)


def setup_inputs(seed: int = 0) -> dict:
    key_of = jax.random.split(jax.random.key(seed), 19)
    tokens = noise(key_of[0], (TOKENS, D), 1.0, 6.0, ((0, 64),))
    norm_gain = jnp.clip(1.0 + 0.18 * jax.random.normal(key_of[1], (D,), jnp.float32), 0.1, 1.9)
    w_query = draw_w_query(jax.random.fold_in(key_of[18], 71), 0)
    w_key = draw_w_key(jax.random.fold_in(key_of[18], 71), 0)
    w_value = noise(key_of[4], (D, KVH * HEAD), D ** -0.5, 0.09375, ((0, 64), (1, 8)))
    w_state_in = noise(key_of[5], (D, ATTN), D ** -0.5, 0.09375, ((0, 64), (1, 8)))
    sink_logit = jnp.clip(2.0 + 4.0 * jax.random.uniform(key_of[6], (QH,), jnp.float32) ** levels(key_of[6], (QH,), ((0, 8),), -0.2, 0.2), 2.0, 6.0)
    decay_rate = draw_decay_rate(jax.random.fold_in(key_of[18], 71), 0)
    rotation = jnp.clip(1.0 + 59.0 * jax.random.uniform(key_of[8], (GROUPS, STATE), jnp.float32) ** levels(key_of[8], (GROUPS, STATE), ((0, 8),), -0.2, 0.2), 1.0, 60.0)
    log_step = jnp.clip(-5.3 + 2.3000002 * jax.random.uniform(key_of[9], (GROUPS,), jnp.float32) ** levels(key_of[9], (GROUPS,), ((0, 8),), -0.2, 0.2), -5.3, -3.0)
    in_re = noise(key_of[10], (GROUPS, STATE, GSIZE), GSIZE ** -0.5, 1.5, ((0, 8),), jnp.float32)
    in_im = noise(key_of[11], (GROUPS, STATE, GSIZE), GSIZE ** -0.5, 1.5, ((0, 8),), jnp.float32)
    out_re = noise(key_of[12], (GROUPS, GSIZE, STATE), STATE ** -0.5, 0.75, ((0, 8),), jnp.float32)
    out_im = noise(key_of[13], (GROUPS, GSIZE, STATE), STATE ** -0.5, 0.75, ((0, 8),), jnp.float32)
    skip_gain = noise(key_of[14], (ATTN,), 1.0, 4.0, ((0, 8),), jnp.float32)
    w_attn_out = noise(key_of[15], (ATTN, D), (ATTN // 16) ** -0.5, 0.5, ((0, 8), (1, 64)))
    w_state_out = noise(key_of[16], (ATTN, D), ATTN ** -0.5, 0.125, ((0, 8), (1, 64)))
    out_gain = jnp.clip(1.0 + 0.18 * jax.random.normal(key_of[17], (D,), jnp.float32), 0.1, 1.9)
    return {"tokens": tokens, "norm_gain": norm_gain, "w_query": w_query, "w_key": w_key, "w_value": w_value, "w_state_in": w_state_in, "sink_logit": sink_logit, "decay_rate": decay_rate, "rotation": rotation, "log_step": log_step, "in_re": in_re, "in_im": in_im, "out_re": out_re, "out_im": out_im, "skip_gain": skip_gain, "w_attn_out": w_attn_out, "w_state_out": w_state_out, "out_gain": out_gain}


epsilon = 1e-06
rotary_base = 500000.0

def rotate(heads_block, positions):
    head_width = heads_block.shape[-1]
    half_width = head_width // 2
    frequency = rotary_base ** (-(jnp.arange(half_width, dtype=jnp.float32) * 2.0 / head_width))
    angles = positions.astype(jnp.float32)[:, None] * frequency[None, :]
    cosine = jnp.cos(angles)[:, None, :]
    sine_part = jnp.sin(angles)[:, None, :]
    lower_half = heads_block[..., :half_width]
    upper_half = heads_block[..., half_width:]
    return jnp.concatenate([lower_half * cosine - upper_half * sine_part, upper_half * cosine + lower_half * sine_part], axis=-1)

def shape_heads(query_sum, key_sum, value_sum, positions, head_width):
    row_count = query_sum.shape[0]
    kv_heads = key_sum.shape[1] // head_width
    group_size = query_sum.shape[1] // key_sum.shape[1]
    queries = rotate(query_sum.reshape(row_count, kv_heads * group_size, head_width), positions).astype(jnp.bfloat16)
    queries = queries.reshape(row_count, kv_heads, group_size, head_width)
    key_rows = rotate(key_sum.reshape(row_count, kv_heads, head_width), positions).astype(jnp.bfloat16)
    key_rows = key_rows.reshape(row_count, kv_heads * head_width)
    value_rows = value_sum.astype(jnp.bfloat16)
    return (queries, key_rows, value_rows)

def band_attention(queries, key_rows, value_rows, sink_logit, first_row, window):
    row_count, kv_heads, group_size, head_width = queries.shape
    blocks = row_count // window
    query_blocks = queries.reshape(blocks, window, kv_heads, group_size, head_width).astype(jnp.float32)
    key_blocks = jnp.concatenate([key_rows[:row_count].reshape(blocks, window, kv_heads, head_width), key_rows[window:].reshape(blocks, window, kv_heads, head_width)], axis=1)
    value_blocks = jnp.concatenate([value_rows[:row_count].reshape(blocks, window, kv_heads, head_width), value_rows[window:].reshape(blocks, window, kv_heads, head_width)], axis=1)
    scores = jnp.einsum('bqkgd,bskd->bkgqs', query_blocks, key_blocks.astype(jnp.float32)) / math.sqrt(head_width)
    block_start = jnp.arange(blocks, dtype=jnp.int32)[:, None, None] * window
    query_at = first_row + block_start + jnp.arange(window, dtype=jnp.int32)[None, :, None]
    key_at = first_row - window + block_start + jnp.arange(2 * window, dtype=jnp.int32)[None, None, :]
    offset_gap = query_at - key_at
    visible = (offset_gap >= 0) & (offset_gap < window) & (key_at >= 0)
    scores = jnp.where(visible[:, None, None, :, :], scores, -jnp.inf)
    sink_value = sink_logit.astype(jnp.float32).reshape(1, kv_heads, group_size, 1, 1)
    top_score = jnp.maximum(lax.optimization_barrier(jnp.max(scores, axis=-1, keepdims=True)), sink_value)
    exponent = jnp.exp(scores - top_score)
    totals = lax.optimization_barrier(jnp.sum(exponent, axis=-1, keepdims=True)) + jnp.exp(sink_value - top_score)
    weights = (exponent / totals).astype(jnp.bfloat16)
    attended = jnp.einsum('bkgqs,bskd->bqkgd', weights.astype(jnp.float32), value_blocks.astype(jnp.float32))
    return attended.reshape(row_count, kv_heads * group_size * head_width).astype(jnp.bfloat16)

def discretize(decay_rate, rotation, log_step, in_re, in_im):
    time_step = jnp.exp(log_step)[:, None]
    lambda_re = -decay_rate
    lambda_im = rotation
    modulus = jnp.exp(lambda_re * time_step)
    pole_re = modulus * jnp.cos(lambda_im * time_step)
    pole_im = modulus * jnp.sin(lambda_im * time_step)
    minus_one = pole_re - 1.0
    denominator = lambda_re * lambda_re + lambda_im * lambda_im
    factor_re = ((minus_one * lambda_re + pole_im * lambda_im) / denominator)[..., None]
    factor_im = ((pole_im * lambda_re - minus_one * lambda_im) / denominator)[..., None]
    drive_re = factor_re * in_re - factor_im * in_im
    drive_im = factor_re * in_im + factor_im * in_re
    return (pole_re, pole_im, drive_re, drive_im)

def chain_link(earlier, later):
    early_are, early_aim, early_bre, early_bim = earlier
    late_are, late_aim, late_bre, late_bim = later
    return (late_are * early_are - late_aim * early_aim, late_are * early_aim + late_aim * early_are, late_are * early_bre - late_aim * early_bim + late_bre, late_are * early_bim + late_aim * early_bre + late_bim)

def local_states(inputs, pole_re, pole_im, drive_re, drive_im):
    row_count = inputs.shape[0]
    groups, states, group_width = drive_re.shape
    channel_values = inputs.astype(jnp.float32).reshape(row_count, groups, group_width)
    push_re = jnp.einsum('tgh,gph->tgp', channel_values, drive_re, precision=lax.Precision.HIGHEST).reshape(row_count, groups * states)
    push_im = jnp.einsum('tgh,gph->tgp', channel_values, drive_im, precision=lax.Precision.HIGHEST).reshape(row_count, groups * states)
    decay_re = jnp.broadcast_to(pole_re.reshape(1, groups * states), push_re.shape)
    decay_im = jnp.broadcast_to(pole_im.reshape(1, groups * states), push_im.shape)
    return lax.associative_scan(chain_link, (decay_re, decay_im, push_re, push_im), axis=0)

def apply_carry(running, carry_re, carry_im):
    power_re, power_im, own_re, own_im = running
    return (own_re + power_re * carry_re - power_im * carry_im, own_im + power_re * carry_im + power_im * carry_re)

def read_out(inputs, state_re, state_im, out_re, out_im, skip_gain):
    row_count = inputs.shape[0]
    groups, group_width, states = out_re.shape
    grid_re = state_re.reshape(row_count, groups, states)
    grid_im = state_im.reshape(row_count, groups, states)
    summed = jnp.einsum('tgp,ghp->tgh', grid_re, out_re, precision=lax.Precision.HIGHEST) - jnp.einsum('tgp,ghp->tgh', grid_im, out_im, precision=lax.Precision.HIGHEST)
    summed = summed.reshape(row_count, groups * group_width) + skip_gain * inputs.astype(jnp.float32)
    return jax.nn.gelu(summed).astype(jnp.bfloat16)

def reference(tokens, norm_gain, w_query, w_key, w_value, w_state_in, sink_logit, decay_rate, rotation, log_step, in_re, in_im, out_re, out_im, skip_gain, w_attn_out, w_state_out, out_gain):
    wide_tokens = tokens.astype(jnp.float32)
    normed = (wide_tokens * lax.rsqrt(lax.optimization_barrier(jnp.mean(wide_tokens * wide_tokens, axis=-1, keepdims=True)) + epsilon) * norm_gain).astype(jnp.bfloat16)
    positions = jnp.arange(TOKENS, dtype=jnp.int32)
    query_sum = jnp.dot(normed, w_query, preferred_element_type=jnp.float32)
    key_sum = jnp.dot(normed, w_key, preferred_element_type=jnp.float32)
    value_sum = jnp.dot(normed, w_value, preferred_element_type=jnp.float32)
    queries, key_rows, value_rows = shape_heads(query_sum, key_sum, value_sum, positions, HEAD)
    inputs = jnp.dot(normed, w_state_in, preferred_element_type=jnp.float32).astype(jnp.bfloat16)
    padded_keys = jnp.concatenate([jnp.zeros((WINDOW, KVH * HEAD), jnp.bfloat16), key_rows], axis=0)
    padded_values = jnp.concatenate([jnp.zeros((WINDOW, KVH * HEAD), jnp.bfloat16), value_rows], axis=0)

    def span_attend(span_index):
        first_row = (span_index * TOK_DEV).astype(jnp.int32)
        span_queries = lax.dynamic_slice_in_dim(queries, first_row, TOK_DEV, 0)
        span_keys = lax.dynamic_slice_in_dim(padded_keys, first_row, TOK_DEV + WINDOW, 0).reshape(TOK_DEV + WINDOW, KVH, HEAD)
        span_values = lax.dynamic_slice_in_dim(padded_values, first_row, TOK_DEV + WINDOW, 0).reshape(TOK_DEV + WINDOW, KVH, HEAD)
        return band_attention(span_queries, span_keys, span_values, sink_logit, first_row, WINDOW)
    attended = lax.map(span_attend, jnp.arange(N_SP, dtype=jnp.int32)).reshape(TOKENS, ATTN)
    pole_re, pole_im, drive_re, drive_im = discretize(decay_rate, rotation, log_step, in_re, in_im)
    spans = inputs.reshape(N_SP, TOK_DEV, ATTN)

    def span_step(carried, span_inputs):
        running = local_states(span_inputs, pole_re, pole_im, drive_re, drive_im)
        state_re, state_im = apply_carry(running, carried[0], carried[1])
        out_rows = read_out(span_inputs, state_re, state_im, out_re, out_im, skip_gain)
        return ((state_re[-1], state_im[-1]), out_rows)
    start_state = (jnp.zeros((GROUPS * STATE,), jnp.float32), jnp.zeros((GROUPS * STATE,), jnp.float32))
    final_state, mixed_spans = lax.scan(span_step, start_state, spans)
    mixed_state = mixed_spans.reshape(TOKENS, ATTN)
    block_width = ATTN // N_TP
    projected = jnp.zeros((TOKENS, D), jnp.float32)
    for block_index in range(N_TP):
        low = block_index * block_width
        partial_term = jnp.dot(attended[:, low:low + block_width], w_attn_out[low:low + block_width], preferred_element_type=jnp.float32) + jnp.dot(mixed_state[:, low:low + block_width], w_state_out[low:low + block_width], preferred_element_type=jnp.float32)
        rounded = lax.optimization_barrier(partial_term.astype(jnp.bfloat16))
        projected = projected + rounded.astype(jnp.float32)
    row_scale = lax.rsqrt(lax.optimization_barrier(jnp.mean(projected * projected, axis=-1, keepdims=True)) + epsilon)
    return (projected * row_scale * out_gain).astype(jnp.bfloat16)
```

```python
import math

import jax
import jax.numpy as jnp
from jax import lax
from jax.experimental import pallas as pl
from jax.experimental.pallas import tpu as pltpu
from jax.sharding import PartitionSpec as P

MESH = pl.DeviceIdType.MESH
F32 = jnp.float32
BF16 = jnp.bfloat16
EPS = 1e-06
BASE = 500000.0
RING = 8
TP = 8
ROWS = 128
D = 4096
NIN = 640
NST = 1024
FLOWS = tuple((half, side) for half in (0, 1) for side in (0, 1))


def nn(a, b):
    return lax.dot_general(a, b, (((1,), (0,)), ((), ())), preferred_element_type=F32)


def nt(a, b):
    return lax.dot_general(a, b, (((1,), (1,)), ((), ())), preferred_element_type=F32)


def split(x):
    high = x.astype(BF16)
    return high, (x - high.astype(F32)).astype(BF16)


def iota(shape, dim):
    return lax.broadcasted_iota(jnp.int32, shape, dim)


def ring(v, d):
    return lax.rem(v + d + 2 * RING, RING)


def cmul(ar, ai, br, bi):
    return ar * br - ai * bi, ar * bi + ai * br


def kernel(
    tok_h, ng_h, wq_h, wk_h, wv_h, ws_h, sink_s, dec_h, rot_h, ls_s,
    inre_h, inim_h, outre_h, outim_h, sg_h, wa_h, wso_h, og_h,
    out_ref,
    W, Wo, tok, xn, kw, vw, ng, og, sg, dec, rot, inre, inim, outre, outim,
    qkvs, cosr, sinr, prow, pw, BDi, BDo, Sr, Si, Er, Ei, Cr, Ci, CY, CZ, KVb, qb, M, Pb, R,
    lsem, w_ssem, w_r1, w_r2, o_ssem, o_r1, o_r2, kv_ss, kv_rs, cy_ss, cy_rs, cz_ss, cz_rs,
    rs_ss, rs_rs,
):
    sp = lax.axis_index("sp")
    t = lax.axis_index("tp")
    z = sp // RING
    y = lax.rem(sp, RING)

    local = [
        (wq_h, W.at[sp, :, pl.ds(0, 256)]),
        (ws_h, W.at[sp, :, pl.ds(256, 256)]),
        (wk_h, kw),
        (wv_h, vw),
        (tok_h, tok),
        (ng_h, ng),
        (dec_h, dec),
        (rot_h, rot),
        (inre_h, inre),
        (inim_h, inim),
        (outre_h, outre),
        (outim_h, outim),
        (wa_h, Wo.at[sp, :, pl.ds(0, 256)]),
        (wso_h, Wo.at[sp, :, pl.ds(256, 256)]),
        (sg_h, sg),
        (og_h, og),
    ]
    copies = [pltpu.make_async_copy(a, b, lsem.at[i]) for i, (a, b) in enumerate(local)]
    for c in copies:
        c.start()

    barrier = pltpu.get_barrier_semaphore()
    after = lax.rem(sp + 1, RING * RING)
    before = lax.rem(sp + RING * RING - 1, RING * RING)
    peers = [(z * RING + ring(y, j), t) for j in range(1, RING)]
    peers += [(ring(z, j) * RING + y, t) for j in range(1, RING)]
    peers += [(sp, lax.rem(t + j, TP)) for j in range(1, TP)]
    peers += [(after, t), (before, t)]
    for peer in peers:
        pl.semaphore_signal(barrier, inc=1, device_id=peer, device_id_type=MESH)

    for i in range(4):
        copies[i].wait()
    lane64 = iota((64, 128), 1)
    row64 = iota((64, 128), 0)
    to_low = (lane64 == row64).astype(F32).astype(BF16)
    to_high = (lane64 == row64 + 64).astype(F32).astype(BF16)
    W[sp, :, 512:640] = (nn(kw[...], to_low) + nn(vw[...], to_high)).astype(BF16)
    pl.semaphore_wait(barrier, len(peers))

    def block(half, d1, d2):
        if half == 0:
            return ring(z, d1) * RING + ring(y, d2)
        return ring(z, d2) * RING + ring(y, d1)

    def neighbour(half, phase, side):
        step = 1 if side == 0 else -1
        if (half == 0) == (phase == 1):
            return (ring(z, step) * RING + y, t)
        return (z * RING + ring(y, step), t)

    def rows(half, hop, side):
        if hop < 4:
            return pl.ds(32 * half, 32)
        return pl.ds(32 * half + 16 * side, 16)

    def piece(buf, ssem, rsem, half, phase, hop, side, index):
        ref = buf.at[index, rows(half, hop, side)]
        return pltpu.make_async_remote_copy(
            src_ref=ref, dst_ref=ref, send_sem=ssem, recv_sem=rsem,
            device_id=neighbour(half, phase, side), device_id_type=MESH,
        )

    def sign(side):
        return 1 if side == 0 else -1

    def offset(k):
        if isinstance(k, int):
            return k // 2 if k % 2 == 0 else -((k + 1) // 2)
        return (1 - 2 * lax.rem(k, 2)) * ((k + 1) // 2)

    class Gather:
        def __init__(self, buf, ssem, r1, r2):
            self.buf, self.ssem, self.r1, self.r2 = buf, ssem, r1, r2

        def first(self, half, side, hop, back):
            index = block(half, -(hop - 1 + back) * sign(side), 0)
            return piece(self.buf, self.ssem, self.r1.at[half, side, hop - 1],
                         half, 1, hop, side, index)

        def second(self, half, side, hop, k, back):
            index = block(half, offset(k), -(hop - 1 + back) * sign(side))
            return piece(self.buf, self.ssem, self.r2.at[half, side, hop - 1, k],
                         half, 2, hop, side, index)

        def begin(self):
            for half, side in FLOWS:
                self.first(half, side, 1, 0).start()

        def own(self, k):
            for half, side in FLOWS:
                self.second(half, side, 1, k, 0).start()

        def stage(self, hop, spread=True):
            for half, side in FLOWS:
                self.first(half, side, hop, 1).wait_recv()
                if hop < 4:
                    self.first(half, side, hop + 1, 0).start()
            if spread:
                self.spread(hop)

        def spread(self, hop):
            self.own(2 * hop - 1)
            if hop < 4:
                self.own(2 * hop)

        def forward(self, hop):
            def step(k, c):
                for half, side in FLOWS:
                    self.second(half, side, hop - 1, k, 1).wait_recv()
                    self.second(half, side, hop, k, 0).start()
                return c
            lax.fori_loop(0, RING, step, 0)

        def last(self):
            def step(k, c):
                for half, side in FLOWS:
                    self.second(half, side, 4, k, 1).wait_recv()
                return c
            lax.fori_loop(0, RING, step, 0)

        def drain(self):
            ref = self.buf.at[pl.ds(0, 63)]
            pltpu.make_async_remote_copy(
                src_ref=ref, dst_ref=ref, send_sem=self.ssem, recv_sem=self.r1.at[0, 0, 0],
                device_id=neighbour(0, 1, 0), device_id_type=MESH,
            ).wait_send()

    win = Gather(W, w_ssem, w_r1, w_r2)
    wout = Gather(Wo, o_ssem, o_r1, o_r2)

    win.begin()
    win.own(0)

    copies[4].wait()
    copies[5].wait()

    def norm_step(i, c):
        at = pl.ds(pl.multiple_of(i * 16, 16), 16)
        x = tok[at, :].astype(F32)
        scale = lax.rsqrt(jnp.mean(x * x, axis=-1, keepdims=True) + EPS)
        xn[at, :] = (x * scale * ng[...]).astype(BF16)
        return c

    lax.fori_loop(0, ROWS // 16, norm_step, 0)
    win.stage(1)

    lane = iota((1, 128), 1)
    freq = jnp.zeros((1, 128), F32)
    for i in range(32):
        freq = jnp.where(lax.rem(lane, 32) == i, F32(BASE ** (-2.0 * i / 64)), freq)
    position = (sp * ROWS + iota((ROWS, 128), 0)).astype(F32)
    angle = position * freq
    lane_full = iota((ROWS, 128), 1)
    low_half = lax.rem(lane_full, 64) < 32
    cosr[...] = jnp.cos(angle)
    sine = jnp.sin(angle)
    sinr[...] = jnp.where(low_half, -sine, sine)
    win.stage(2)

    for i in (6, 7):
        copies[i].wait()
    lane_n = iota((1, NST), 1)
    spread64 = (lax.rem(iota((64, NST), 1), 64) == iota((64, NST), 0)).astype(F32)
    own_group = iota((16, NST), 1) // 64 == iota((16, NST), 0)

    def as_row(ref):
        tiled = lax.dot_general(
            ref[...], spread64, (((1,), (0,)), ((), ())),
            precision=lax.Precision.HIGHEST, preferred_element_type=F32,
        )
        return jnp.sum(jnp.where(own_group, tiled, 0.0), axis=0, keepdims=True)

    lam_re = -as_row(dec)
    lam_im = as_row(rot)
    step_log = jnp.zeros((1, NST), F32)
    for g in range(16):
        step_log = jnp.where(lane_n // 64 == g, ls_s[g], step_log)
    delta = jnp.exp(step_log)
    modulus = jnp.exp(lam_re * delta)
    pr = modulus * jnp.cos(lam_im * delta)
    pi = modulus * jnp.sin(lam_im * delta)
    less = pr - 1.0
    den = lam_re * lam_re + lam_im * lam_im
    prow[0:1, :] = (less * lam_re + pi * lam_im) / den
    prow[1:2, :] = (pi * lam_re - less * lam_im) / den
    ar, ai = pr, pi
    for k in range(16):
        pw[0, k : k + 1, :] = ar
        pw[1, k : k + 1, :] = ai
        if k < 15:
            ar, ai = cmul(ar, ai, pr, pi)
    prow[2:3, :] = ar
    prow[3:4, :] = ai
    for _ in range(3):
        ar, ai = cmul(ar, ai, ar, ai)
    prow[4:5, :] = ar
    prow[5:6, :] = ai
    for _ in range(3):
        ar, ai = cmul(ar, ai, ar, ai)
    prow[6:7, :] = ar
    prow[7:8, :] = ai
    win.stage(3)

    for i in (8, 9, 10, 11):
        copies[i].wait()
    spread64b = spread64.astype(BF16)
    own_block = iota((256, NST), 0) // 16 == iota((256, NST), 1) // 64

    def diagonal(dst, at, value):
        for part, value in enumerate(split(value.reshape(256, 64))):
            dst[at + part] = jnp.where(own_block, nn(value, spread64b), 0.0).astype(BF16)

    diagonal(BDi, 0, inre[...])
    diagonal(BDi, 2, inim[...])
    win.stage(4)
    diagonal(BDo, 0, outre[...])
    diagonal(BDo, 2, -outim[...])

    for i in (12, 13, 14, 15):
        copies[i].wait()

    win.forward(2)
    wout.begin()
    win.forward(3)
    wout.stage(1, False)
    win.forward(4)
    wout.stage(2, False)
    wout.own(0)
    wout.spread(1)
    wout.spread(2)
    win.last()
    wout.stage(3)

    def project(i, c):
        wide = W[pl.ds(pl.multiple_of(i * 8, 8), 8)].reshape(512, NIN)
        xs = xn[:, pl.ds(pl.multiple_of(i * 512, 512), 512)]
        part = nn(xs, wide)

        @pl.when(i == 0)
        def _():
            qkvs[...] = part

        @pl.when(i > 0)
        def _():
            qkvs[...] += part

        return c

    lax.fori_loop(0, RING, project, 0)
    wout.stage(4)

    def swapped(x):
        return jnp.where(low_half, pltpu.roll(x, 96, 1), pltpu.roll(x, 32, 1))

    kv = qkvs[:, 512:640]
    key_lane = lane_full < 64
    kv = kv * jnp.where(key_lane, cosr[...], 1.0) + swapped(kv) * jnp.where(
        key_lane, sinr[...], 0.0
    )
    KVb[1] = kv.astype(BF16)
    u = qkvs[:, 256:512].astype(BF16)
    permute = (
        iota((ROWS, ROWS), 1)
        == 16 * lax.rem(iota((ROWS, ROWS), 0), 8) + iota((ROWS, ROWS), 0) // 8
    ).astype(F32).astype(BF16)
    up = nn(permute, u).astype(BF16)
    kv_copy = pltpu.make_async_remote_copy(
        src_ref=KVb.at[1], dst_ref=KVb.at[0], send_sem=kv_ss, recv_sem=kv_rs,
        device_id=(after, t), device_id_type=MESH,
    )
    kv_copy.start()

    Sr[...] = nn(up, BDi[0]) + nn(up, BDi[1])
    Si[...] = nn(up, BDi[2]) + nn(up, BDi[3])
    fr, fi = prow[0:1, :], prow[1:2, :]
    pr, pi = pw[0, 0:1, :], pw[1, 0:1, :]
    sr = jnp.zeros((8, NST), F32)
    si = jnp.zeros((8, NST), F32)
    for i in range(16):
        at = slice(8 * i, 8 * i + 8)
        br, bi = cmul(fr, fi, Sr[at, :], Si[at, :])
        sr, si = cmul(pr, pi, sr, si)
        sr, si = sr + br, si + bi
        Sr[at, :] = sr
        Si[at, :] = si
    Er[...] = sr
    Ei[...] = si
    qr, qi = prow[2:3, :], prow[3:4, :]
    cr = jnp.zeros((1, NST), F32)
    ci = jnp.zeros((1, NST), F32)
    for j in range(8):
        cr, ci = cmul(qr, qi, cr, ci)
        cr, ci = cr + Er[j : j + 1, :], ci + Ei[j : j + 1, :]
    CY[y, 0:1, :] = cr
    CY[y, 1:2, :] = ci
    for pair in range(2):
        x = qkvs[:, 128 * pair : 128 * pair + 128]
        qb[:, 128 * pair : 128 * pair + 128] = (x * cosr[...] + swapped(x) * sinr[...]).astype(BF16)

    def carry_copy(buf, ss, rs, at, peer):
        return pltpu.make_async_remote_copy(
            src_ref=buf.at[at], dst_ref=buf.at[at], send_sem=ss, recv_sem=rs,
            device_id=peer, device_id_type=MESH,
        )

    def carry_all(buf, ss, rs):
        return carry_copy(buf, ss, rs, pl.ds(0, 7), peers[0])

    for j in range(1, RING):
        carry_copy(CY, cy_ss, cy_rs, y, (z * RING + ring(y, j), t)).start()
    wout.forward(2)

    kv_copy.wait_recv()
    both = KVb[...].reshape(2 * ROWS, 128).astype(F32)
    turned = pltpu.roll(both, 64, 1)
    first_half = iota((2 * ROWS, 128), 1) < 64
    k_low = jnp.where(first_half, both, 0.0).astype(BF16)
    k_high = jnp.where(first_half, 0.0, turned).astype(BF16)
    v_low = jnp.where(first_half, turned, 0.0).astype(BF16)
    v_high = jnp.where(first_half, 0.0, both).astype(BF16)
    gap = iota((ROWS, 2 * ROWS), 0) + ROWS - iota((ROWS, 2 * ROWS), 1)
    key_at = sp * ROWS - ROWS + iota((ROWS, 2 * ROWS), 1)
    visible = (gap >= 0) & (gap < ROWS) & (key_at >= 0)

    def attend(pair):
        q = qb[:, 128 * pair : 128 * pair + 128]
        total = None
        for side, (k, v) in enumerate(((k_low, v_low), (k_high, v_high))):
            score = jnp.where(visible, nt(q, k) * 0.125, -jnp.inf)
            sink = sink_s[2 * pair + side]
            top = jnp.maximum(jnp.max(score, axis=-1, keepdims=True), sink)
            e = jnp.exp(score - top)
            weight = e / (jnp.sum(e, axis=-1, keepdims=True) + jnp.exp(sink - top))
            part = nn(weight.astype(BF16), v)
            total = part if total is None else total + part
        M[:, 128 * pair : 128 * pair + 128] = total.astype(BF16)

    attend(0)

    carry_all(CY, cy_ss, cy_rs).wait_recv()
    br, bi = prow[4:5, :], prow[5:6, :]
    cr = jnp.zeros((1, NST), F32)
    ci = jnp.zeros((1, NST), F32)
    rowr, rowi = cr, ci
    wr, wi = cr + 1.0, ci
    for j in range(RING):
        keep = jnp.where(y == j, 1.0, 0.0).astype(F32)
        rowr = rowr + keep * cr
        rowi = rowi + keep * ci
        cr, ci = cmul(br, bi, cr, ci)
        cr, ci = cr + CY[j, 0:1, :], ci + CY[j, 1:2, :]
        go = jnp.where(y > j, 1.0, 0.0).astype(F32)
        nr, ni = cmul(br, bi, wr, wi)
        wr = wr + go * (nr - wr)
        wi = wi + go * (ni - wi)
    CZ[z, 0:1, :] = cr
    CZ[z, 1:2, :] = ci
    Cr[0:1, :] = rowr
    Ci[0:1, :] = rowi
    Cr[1:2, :] = wr
    Ci[1:2, :] = wi
    for j in range(1, RING):
        carry_copy(CZ, cz_ss, cz_rs, z, (ring(z, j) * RING + y, t)).start()
    wout.forward(3)
    attend(1)

    carry_all(CZ, cz_ss, cz_rs).wait_recv()
    br, bi = prow[6:7, :], prow[7:8, :]
    cr = jnp.zeros((1, NST), F32)
    ci = jnp.zeros((1, NST), F32)
    for j in range(RING - 1):
        go = jnp.where(z > j, 1.0, 0.0).astype(F32)
        nr, ni = cmul(br, bi, cr, ci)
        nr, ni = nr + CZ[j, 0:1, :], ni + CZ[j, 1:2, :]
        cr = go * nr + (1.0 - go) * cr
        ci = go * ni + (1.0 - go) * ci
    cr, ci = cmul(Cr[1:2, :], Ci[1:2, :], cr, ci)
    cr, ci = cr + Cr[0:1, :], ci + Ci[0:1, :]
    for j in range(8):
        Cr[j : j + 1, :] = cr
        Ci[j : j + 1, :] = ci
        cr, ci = cmul(qr, qi, cr, ci)
        cr, ci = cr + Er[j : j + 1, :], ci + Ei[j : j + 1, :]
    cr, ci = Cr[...], Ci[...]
    for i in range(16):
        at = slice(8 * i, 8 * i + 8)
        gr, gi = cmul(pw[0, i : i + 1, :], pw[1, i : i + 1, :], cr, ci)
        Sr[at, :] = Sr[at, :] + gr
        Si[at, :] = Si[at, :] + gi
    total = up.astype(F32) * sg[...]
    for j, ref in ((0, Sr), (2, Si)):
        high, low = split(ref[...])
        total = total + nt(high, BDo[j]) + nt(low, BDo[j]) + nt(high, BDo[j + 1])
    mixed = jax.nn.gelu(total).astype(BF16)
    M[:, 256:512] = lax.dot_general(
        permute, mixed, (((0,), (0,)), ((), ())), preferred_element_type=F32
    ).astype(BF16)

    def chunk(half, a):
        lines = [
            Wo[(8 * j + a) if half == 0 else (8 * a + j), 32 * half : 32 * half + 32]
            for j in range(RING)
        ]
        part = nt(M[...], jnp.concatenate(lines, axis=0)).astype(BF16)
        at = a + RING * half
        Pb[at] = part.reshape(TP, 16, 256)
        R[t, at] = Pb[at, t]
        return at

    def owner_copy(at, j):
        to = lax.rem(t + j, TP)
        return pltpu.make_async_remote_copy(
            src_ref=Pb.at[at, to], dst_ref=R.at[t, at], send_sem=rs_ss, recv_sem=rs_rs,
            device_id=(sp, to), device_id_type=MESH,
        )

    def chunks(items):
        made = [chunk(half, a) for half, a in items]
        for at in made:
            for j in range(1, TP):
                owner_copy(at, j).start()

    def at_hop(hop):
        return [(0, ring(y, hop)), (0, ring(y, -hop)), (1, ring(z, hop)), (1, ring(z, -hop))]

    chunks([(0, y), (1, z)] + at_hop(1))
    wout.forward(4)
    chunks(at_hop(2))
    chunks(at_hop(3))
    wout.last()
    chunks([(0, ring(y, 4)), (1, ring(z, 4))])

    kv_copy.wait_send()
    carry_all(CY, cy_ss, cy_rs).wait_send()
    carry_all(CZ, cz_ss, cz_rs).wait_send()
    win.drain()
    wout.drain()
    whole = pltpu.make_async_remote_copy(
        src_ref=R.at[pl.ds(0, 7)], dst_ref=R.at[pl.ds(0, 7)], send_sem=rs_ss, recv_sem=rs_rs,
        device_id=peers[0], device_id_type=MESH,
    )
    whole.wait_send()
    whole.wait_recv()

    square = jnp.zeros((16, 1), F32)
    sums = []
    for at in range(2 * RING):
        total = R[0, at].astype(F32)
        for j in range(1, TP):
            total = total + R[j, at].astype(F32)
        sums.append(total)
        square = square + jnp.sum(total * total, axis=-1, keepdims=True)
    scale = lax.rsqrt(square * (1.0 / D) + EPS)
    quarter = iota((16, 128), 1) // 32
    for n in range(32):
        zz, y0 = n // 4, 2 * (n % 4)
        tile = None
        pieces = ((sums[y0], zz), (sums[RING + zz], y0), (sums[y0 + 1], zz), (sums[RING + zz], y0 + 1))
        for place, (source, at) in enumerate(pieces):
            part = source[:, 128 * (at // 4) : 128 * (at // 4) + 128]
            shift = (32 * place - 32 * (at % 4)) % 128
            if shift:
                part = pltpu.roll(part, shift, 1)
            tile = part if tile is None else jnp.where(quarter == place, part, tile)
        cols = slice(128 * n, 128 * n + 128)
        out_ref[:, cols] = (tile * scale * og[:, cols]).astype(BF16)


def body(
    tokens, norm_gain, w_query, w_key, w_value, w_state_in, sink_logit, decay_rate, rotation,
    log_step, in_re, in_im, out_re, out_im, skip_gain, w_attn_out, w_state_out, out_gain,
):
    vm, dma = pltpu.VMEM, pltpu.SemaphoreType.DMA
    spec = pl.BlockSpec(memory_space=pl.ANY)
    specs = [spec] * 18
    specs[6] = specs[9] = pl.BlockSpec(memory_space=pltpu.SMEM)
    return pl.pallas_call(
        kernel,
        out_shape=jax.ShapeDtypeStruct((16, D), BF16),
        in_specs=specs,
        out_specs=pl.BlockSpec(memory_space=pltpu.VMEM),
        scratch_shapes=[
            vm((64, 64, NIN), BF16),
            vm((64, 64, 512), BF16),
            vm((ROWS, D), BF16),
            vm((ROWS, D), BF16),
            vm((64, 64), BF16),
            vm((64, 64), BF16),
            vm((1, D), F32),
            vm((1, D), F32),
            vm((1, 256), F32),
            vm((16, 64), F32),
            vm((16, 64), F32),
            vm((16, 16, 64), F32),
            vm((16, 16, 64), F32),
            vm((16, 16, 64), F32),
            vm((16, 16, 64), F32),
            vm((ROWS, NIN), F32),
            vm((ROWS, 128), F32),
            vm((ROWS, 128), F32),
            vm((8, NST), F32),
            vm((2, 16, NST), F32),
            vm((4, 256, NST), BF16),
            vm((4, 256, NST), BF16),
            vm((ROWS, NST), F32),
            vm((ROWS, NST), F32),
            vm((8, NST), F32),
            vm((8, NST), F32),
            vm((8, NST), F32),
            vm((8, NST), F32),
            vm((RING, 2, NST), F32),
            vm((RING, 2, NST), F32),
            vm((2, ROWS, 128), BF16),
            vm((ROWS, 256), BF16),
            vm((ROWS, 512), BF16),
            vm((2 * RING, TP, 16, 256), BF16),
            vm((TP, 2 * RING, 16, 256), BF16),
            dma((16,)),
            dma, dma((2, 2, 4)), dma((2, 2, 4, RING)),
            dma, dma((2, 2, 4)), dma((2, 2, 4, RING)),
            dma, dma, dma, dma, dma, dma, dma, dma,
        ],
        compiler_params=pltpu.CompilerParams(collective_id=0, has_side_effects=True),
    )(
        tokens, norm_gain.reshape(1, D), w_query, w_key, w_value, w_state_in, sink_logit,
        decay_rate, rotation, log_step, in_re.transpose(0, 2, 1), in_im.transpose(0, 2, 1),
        out_re, out_im, skip_gain.reshape(1, 256), w_attn_out.T, w_state_out.T, out_gain.reshape(1, D),
    )


def solution(mesh):
    return jax.shard_map(
        body,
        mesh=mesh,
        in_specs=(
            P("sp", None),
            P(),
            P("sp", "tp"),
            P("sp", "tp"),
            P("sp", "tp"),
            P("sp", "tp"),
            P("tp"),
            P("tp", None),
            P("tp", None),
            P("tp"),
            P("tp", None, None),
            P("tp", None, None),
            P("tp", None, None),
            P("tp", None, None),
            P("tp"),
            P("tp", "sp"),
            P("tp", "sp"),
            P(),
        ),
        out_specs=P(("sp", "tp"), None),
        check_vma=False,
    )
```

```python
import math

import jax
import jax.numpy as jnp
from jax import lax
from jax.experimental import pallas as pl
from jax.experimental.pallas import tpu as pltpu
from jax.sharding import PartitionSpec as P

MESH = pl.DeviceIdType.MESH
F32 = jnp.float32
BF16 = jnp.bfloat16
EPS = 1e-06
BASE = 500000.0
RING = 8
TP = 8
CHIPS = 4
ROWS = 128
D = 4096
NIN = 640
NST = 1024
FLOWS = tuple((half, side) for half in (0, 1) for side in (0, 1))


def nn(a, b):
    return lax.dot_general(a, b, (((1,), (0,)), ((), ())), preferred_element_type=F32)


def nt(a, b):
    return lax.dot_general(a, b, (((1,), (1,)), ((), ())), preferred_element_type=F32)


def split(x):
    high = x.astype(BF16)
    return high, (x - high.astype(F32)).astype(BF16)


def iota(shape, dim):
    return lax.broadcasted_iota(jnp.int32, shape, dim)


def ring(v, d):
    return lax.rem(v + d + 2 * RING, RING)


def cmul(ar, ai, br, bi):
    return ar * br - ai * bi, ar * bi + ai * br


def kernel(
    tok_h, ng_h, wq_h, wk_h, wv_h, ws_h, sink_h, dec_h, rot_h, ls_h,
    inre_h, inim_h, outre_h, outim_h, sg_h, wa_h, wso_h, og_h,
    out_ref,
    W, Wo, tok, xn, xh, kw, vw, sink_s, ls_s, ng, og, sg, dec, rot, inre, inim, outre, outim,
    qkvs, cosr, sinr, prow, pw, BDi, BDo, Sr, Si, Er, Ei, Cr, Ci, CY, CZ, KVb, qb, M, PP, PR, Pb, R, T,
    lsem, w_ssem, w_r1, w_r2, o_ssem, o_r1, o_r2, kv_ss, kv_rs, cy_ss, cy_rs, cz_ss, cz_rs,
    rs_ss, rs_rs, tw_ss, tw_rs,
):
    sp = lax.axis_index("sp")
    t = lax.axis_index("tp")
    z = sp // RING
    y = lax.rem(sp, RING)

    chip = t // 2
    core = lax.rem(t, 2)
    twin = (sp, t + 1 - 2 * core)
    barrier = pltpu.get_barrier_semaphore()
    after = lax.rem(sp + 1, RING * RING)
    before = lax.rem(sp + RING * RING - 1, RING * RING)
    peers = [(z * RING + ring(y, j), t) for j in range(1, RING)]
    peers += [(ring(z, j) * RING + y, t) for j in range(1, RING)]
    peers += [(sp, lax.rem(t + 2 * j, TP)) for j in range(1, CHIPS)]
    peers += [twin]
    peers += [(after, t), (before, t)]
    for peer in peers:
        pl.semaphore_signal(barrier, inc=1, device_id=peer, device_id_type=MESH)

    mine = (y * RING + z, z * RING + y)
    local = []
    for half in (0, 1):
        at = pl.ds(32 * half, 32)
        local += [
            (wq_h.at[at], W.at[half, mine[half], :, pl.ds(0, 256)]),
            (ws_h.at[at], W.at[half, mine[half], :, pl.ds(256, 256)]),
        ]
    local += [
        (wk_h, kw),
        (wv_h, vw),
        (tok_h, tok),
        (ng_h, ng),
        (dec_h, dec),
        (rot_h, rot),
        (inre_h, inre),
        (inim_h, inim),
        (outre_h, outre),
        (outim_h, outim),
        (sg_h, sg),
        (og_h, og),
        (sink_h, sink_s),
        (ls_h, ls_s),
    ]
    for half in (0, 1):
        at = pl.ds(32 * half, 32)
        local += [
            (wa_h.at[at], Wo.at[half, mine[half], :, pl.ds(0, 256)]),
            (wso_h.at[at], Wo.at[half, mine[half], :, pl.ds(256, 256)]),
        ]
    copies = [pltpu.make_async_copy(a, b, lsem.at[i]) for i, (a, b) in enumerate(local)]
    for c in copies:
        c.start()

    for i in range(6):
        copies[i].wait()
    lane64 = iota((64, 128), 1)
    row64 = iota((64, 128), 0)
    to_low = (lane64 == row64).astype(F32).astype(BF16)
    to_high = (lane64 == row64 + 64).astype(F32).astype(BF16)
    kv_part = (nn(kw[...], to_low) + nn(vw[...], to_high)).astype(BF16)
    W[0, mine[0], :, 512:640] = kv_part[:32]
    W[1, mine[1], :, 512:640] = kv_part[32:]
    pl.semaphore_wait(barrier, len(peers))

    def block(half, d1, d2):
        first, second = (z, y) if half == 0 else (y, z)
        return ring(second, d2) * RING + ring(first, d1)

    def neighbour(half, phase, side):
        step = 1 if side == 0 else -1
        if (half == 0) == (phase == 1):
            return (ring(z, step) * RING + y, t)
        return (z * RING + ring(y, step), t)

    def rows(hop, side):
        return pl.ds(0, 32) if hop < 4 else pl.ds(16 * side, 16)

    def piece(buf, ssem, rsem, half, phase, hop, side, index):
        ref = buf.at[half, index, rows(hop, side)]
        return pltpu.make_async_remote_copy(
            src_ref=ref, dst_ref=ref, send_sem=ssem, recv_sem=rsem,
            device_id=neighbour(half, phase, side), device_id_type=MESH,
        )

    def sign(side):
        return 1 if side == 0 else -1

    def offset(k):
        if isinstance(k, int):
            return k // 2 if k % 2 == 0 else -((k + 1) // 2)
        return (1 - 2 * lax.rem(k, 2)) * ((k + 1) // 2)

    class Gather:
        def __init__(self, buf, ssem, r1, r2):
            self.buf, self.ssem, self.r1, self.r2 = buf, ssem, r1, r2

        def first(self, half, side, hop, back):
            index = block(half, -(hop - 1 + back) * sign(side), 0)
            return piece(self.buf, self.ssem, self.r1.at[half, side, hop - 1],
                         half, 1, hop, side, index)

        def second(self, half, side, hop, k, back):
            index = block(half, offset(k), -(hop - 1 + back) * sign(side))
            return piece(self.buf, self.ssem, self.r2.at[half, side, hop - 1, k],
                         half, 2, hop, side, index)

        def begin(self):
            for half, side in FLOWS:
                self.first(half, side, 1, 0).start()

        def own(self, k):
            for half, side in FLOWS:
                self.second(half, side, 1, k, 0).start()

        def stage(self, hop, spread=True):
            for half, side in FLOWS:
                self.first(half, side, hop, 1).wait_recv()
                if hop < 4:
                    self.first(half, side, hop + 1, 0).start()
            if spread:
                self.spread(hop)

        def spread(self, hop):
            self.own(2 * hop - 1)
            if hop < 4:
                self.own(2 * hop)

        def forward(self, hop, begin=0, end=RING):
            def step(k, c):
                for half, side in FLOWS:
                    self.second(half, side, hop - 1, k, 1).wait_recv()
                    self.second(half, side, hop, k, 0).start()
                return c
            lax.fori_loop(begin, end, step, 0)

        def last(self):
            def step(k, c):
                for half, side in FLOWS:
                    self.second(half, side, 4, k, 1).wait_recv()
                return c
            lax.fori_loop(0, RING, step, 0)

        def drain(self):
            ref = self.buf.at[:, pl.ds(0, 63)]
            pltpu.make_async_remote_copy(
                src_ref=ref, dst_ref=ref, send_sem=self.ssem, recv_sem=self.r1.at[0, 0, 0],
                device_id=neighbour(0, 1, 0), device_id_type=MESH,
            ).wait_send()

    win = Gather(W, w_ssem, w_r1, w_r2)
    wout = Gather(Wo, o_ssem, o_r1, o_r2)

    for i in (18, 19, 20, 21):
        copies[i].wait()
    for gather in (win, wout):
        gather.begin()
        gather.own(0)

    copies[6].wait()
    copies[7].wait()

    def norm_step(i, c):
        at = pl.ds(pl.multiple_of(i * 16, 16), 16)
        x = tok[at, :].astype(F32)
        scale = lax.rsqrt(jnp.mean(x * x, axis=-1, keepdims=True) + EPS)
        xn[at, :] = (x * scale * ng[...]).astype(BF16)
        return c

    lax.fori_loop(0, ROWS // 16, norm_step, 0)
    win.stage(1)
    win.forward(2, 0, 1)

    lane = iota((1, 128), 1)
    freq = jnp.zeros((1, 128), F32)
    for i in range(32):
        freq = jnp.where(lax.rem(lane, 32) == i, F32(BASE ** (-2.0 * i / 64)), freq)
    position = (sp * ROWS + iota((ROWS, 128), 0)).astype(F32)
    angle = position * freq
    lane_full = iota((ROWS, 128), 1)
    low_half = lax.rem(lane_full, 64) < 32
    cosr[...] = jnp.cos(angle)
    sine = jnp.sin(angle)
    sinr[...] = jnp.where(low_half, -sine, sine)
    win.stage(2)
    wout.stage(1, False)
    win.forward(2, 1, 2)

    lane128 = iota((ROWS, 128), 1) // 32
    source = iota((512, 256), 0)
    target = iota((512, 256), 1)
    spot = 64 * (target // 32) + lax.rem(target, 32)
    picks = [(source == spot + 32 * half).astype(F32).astype(BF16) for half in (0, 1)]
    for i in range(RING):
        xh[1, i] = nn(xn[:, 512 * i : 512 * i + 512], picks[1]).astype(BF16)
    for group in range(2):
        rolled = []
        for i in range(4):
            at = 512 * (4 * group + i)
            part = nn(xn[:, at : at + 512], picks[0])
            rolled.append((part[:, :128], part[:, 128:]))
        for j in range(RING):
            tile = None
            for i in range(4):
                part = rolled[i][j // 4]
                shift = 32 * ((i - j) % 4)
                if shift:
                    part = pltpu.roll(part, shift, 1)
                tile = part if tile is None else jnp.where(lane128 == i, part, tile)
            xh[0, j, :, 128 * group : 128 * group + 128] = tile.astype(BF16)

    for i in (8, 9, 17):
        copies[i].wait()
    lane_n = iota((1, NST), 1)
    spread64 = (lax.rem(iota((64, NST), 1), 64) == iota((64, NST), 0)).astype(F32)
    own_group = iota((16, NST), 1) // 64 == iota((16, NST), 0)

    def as_row(ref):
        tiled = lax.dot_general(
            ref[...], spread64, (((1,), (0,)), ((), ())),
            precision=lax.Precision.HIGHEST, preferred_element_type=F32,
        )
        return jnp.sum(jnp.where(own_group, tiled, 0.0), axis=0, keepdims=True)

    lam_re = -as_row(dec)
    lam_im = as_row(rot)
    step_log = jnp.zeros((1, NST), F32)
    for g in range(16):
        step_log = jnp.where(lane_n // 64 == g, ls_s[g], step_log)
    delta = jnp.exp(step_log)
    modulus = jnp.exp(lam_re * delta)
    pr = modulus * jnp.cos(lam_im * delta)
    pi = modulus * jnp.sin(lam_im * delta)
    less = pr - 1.0
    den = lam_re * lam_re + lam_im * lam_im
    prow[0:1, :] = (less * lam_re + pi * lam_im) / den
    prow[1:2, :] = (pi * lam_re - less * lam_im) / den
    ar, ai = pr, pi
    for k in range(16):
        pw[0, k : k + 1, :] = ar
        pw[1, k : k + 1, :] = ai
        if k < 15:
            ar, ai = cmul(ar, ai, pr, pi)
    prow[2:3, :] = ar
    prow[3:4, :] = ai
    for _ in range(3):
        ar, ai = cmul(ar, ai, ar, ai)
    prow[4:5, :] = ar
    prow[5:6, :] = ai
    for _ in range(3):
        ar, ai = cmul(ar, ai, ar, ai)
    prow[6:7, :] = ar
    prow[7:8, :] = ai
    win.stage(3)
    win.forward(2, 2, 4)

    for i in (10, 11, 12, 13):
        copies[i].wait()
    spread64b = spread64.astype(BF16)
    own_block = iota((256, NST), 0) // 16 == iota((256, NST), 1) // 64

    def diagonal(dst, at, value):
        for part, value in enumerate(split(value.reshape(256, 64))):
            dst[at + part] = jnp.where(own_block, nn(value, spread64b), 0.0).astype(BF16)

    diagonal(BDi, 0, inre[...])
    diagonal(BDi, 2, inim[...])
    win.stage(4)
    win.forward(2, 4, 6)
    diagonal(BDo, 0, outre[...])
    diagonal(BDo, 2, -outim[...])

    for i in (14, 15, 16):
        copies[i].wait()
    win.forward(2, 6, 8)
    wout.stage(2, False)

    def project(half, a, fresh=False):
        wide = W[half, pl.ds(pl.multiple_of(a * RING, RING), RING)].reshape(256, NIN)
        part = nn(xh[half, a], wide)
        qkvs[...] = part if fresh else qkvs[...] + part

    def at_hop(hop):
        if hop == 0:
            return [(0, y), (1, z)]
        if hop == 4:
            return [(0, ring(y, 4)), (1, ring(z, 4))]
        return [(0, ring(y, hop)), (0, ring(y, -hop)), (1, ring(z, hop)), (1, ring(z, -hop))]

    def projects(hop):
        for n, (half, a) in enumerate(at_hop(hop)):
            project(half, a, hop == 0 and n == 0)

    projects(0)
    win.forward(3, 0, 4)
    projects(1)
    win.forward(3, 4, 8)
    wout.stage(3, False)
    win.forward(4, 0, 4)
    projects(2)
    win.forward(4, 4, 8)
    wout.stage(4, False)
    for k in range(1, RING):
        wout.own(k)
    projects(3)
    win.last()
    projects(4)

    def swapped(x):
        return jnp.where(low_half, pltpu.roll(x, 96, 1), pltpu.roll(x, 32, 1))

    kv = qkvs[:, 512:640]
    key_lane = lane_full < 64
    kv = kv * jnp.where(key_lane, cosr[...], 1.0) + swapped(kv) * jnp.where(
        key_lane, sinr[...], 0.0
    )
    KVb[1] = kv.astype(BF16)
    kv_copy = pltpu.make_async_remote_copy(
        src_ref=KVb.at[1], dst_ref=KVb.at[0], send_sem=kv_ss, recv_sem=kv_rs,
        device_id=(after, t), device_id_type=MESH,
    )
    kv_copy.start()

    wout.forward(2, 0, 2)

    u = qkvs[:, 256:512].astype(BF16)
    permute = (
        iota((ROWS, ROWS), 1)
        == 16 * lax.rem(iota((ROWS, ROWS), 0), 8) + iota((ROWS, ROWS), 0) // 8
    ).astype(F32).astype(BF16)
    up = nn(permute, u).astype(BF16)
    Sr[...] = nn(up, BDi[0]) + nn(up, BDi[1])
    Si[...] = nn(up, BDi[2]) + nn(up, BDi[3])
    fr, fi = prow[0:1, :], prow[1:2, :]
    pr, pi = pw[0, 0:1, :], pw[1, 0:1, :]
    sr = jnp.zeros((8, NST), F32)
    si = jnp.zeros((8, NST), F32)
    for i in range(16):
        at = slice(8 * i, 8 * i + 8)
        br, bi = cmul(fr, fi, Sr[at, :], Si[at, :])
        sr, si = cmul(pr, pi, sr, si)
        sr, si = sr + br, si + bi
        Sr[at, :] = sr
        Si[at, :] = si
    Er[...] = sr
    Ei[...] = si
    qr, qi = prow[2:3, :], prow[3:4, :]
    cr = jnp.zeros((1, NST), F32)
    ci = jnp.zeros((1, NST), F32)
    for j in range(8):
        cr, ci = cmul(qr, qi, cr, ci)
        cr, ci = cr + Er[j : j + 1, :], ci + Ei[j : j + 1, :]
    CY[y, 0:1, :] = cr
    CY[y, 1:2, :] = ci

    def carry_copy(buf, ss, rs, at, peer):
        return pltpu.make_async_remote_copy(
            src_ref=buf.at[at], dst_ref=buf.at[at], send_sem=ss, recv_sem=rs,
            device_id=peer, device_id_type=MESH,
        )

    def carry_all(buf, ss, rs):
        return carry_copy(buf, ss, rs, pl.ds(0, 7), peers[0])

    for j in range(1, RING):
        carry_copy(CY, cy_ss, cy_rs, y, (z * RING + ring(y, j), t)).start()
    wout.forward(2, 2, 6)
    for pair in range(2):
        x = qkvs[:, 128 * pair : 128 * pair + 128]
        qb[:, 128 * pair : 128 * pair + 128] = (x * cosr[...] + swapped(x) * sinr[...]).astype(BF16)
    wout.forward(2, 6, 8)

    kv_copy.wait_recv()
    both = KVb[...].reshape(2 * ROWS, 128).astype(F32)
    turned = pltpu.roll(both, 64, 1)
    first_half = iota((2 * ROWS, 128), 1) < 64
    k_low = jnp.where(first_half, both, 0.0).astype(BF16)
    k_high = jnp.where(first_half, 0.0, turned).astype(BF16)
    v_low = jnp.where(first_half, turned, 0.0).astype(BF16)
    v_high = jnp.where(first_half, 0.0, both).astype(BF16)
    gap = iota((ROWS, 2 * ROWS), 0) + ROWS - iota((ROWS, 2 * ROWS), 1)
    key_at = sp * ROWS - ROWS + iota((ROWS, 2 * ROWS), 1)
    visible = (gap >= 0) & (gap < ROWS) & (key_at >= 0)

    def attend(pair):
        q = qb[:, 128 * pair : 128 * pair + 128]
        total = None
        for side, (k, v) in enumerate(((k_low, v_low), (k_high, v_high))):
            score = jnp.where(visible, nt(q, k) * 0.125, -jnp.inf)
            sink = sink_s[2 * pair + side]
            top = jnp.maximum(jnp.max(score, axis=-1, keepdims=True), sink)
            e = jnp.exp(score - top)
            weight = e / (jnp.sum(e, axis=-1, keepdims=True) + jnp.exp(sink - top))
            part = nn(weight.astype(BF16), v)
            total = part if total is None else total + part
        M[:, 128 * pair : 128 * pair + 128] = total.astype(BF16)


    attend(0)
    carry_all(CY, cy_ss, cy_rs).wait_recv()
    br, bi = prow[4:5, :], prow[5:6, :]
    cr = jnp.zeros((1, NST), F32)
    ci = jnp.zeros((1, NST), F32)
    rowr, rowi = cr, ci
    wr, wi = cr + 1.0, ci
    for j in range(RING):
        keep = jnp.where(y == j, 1.0, 0.0).astype(F32)
        rowr = rowr + keep * cr
        rowi = rowi + keep * ci
        cr, ci = cmul(br, bi, cr, ci)
        cr, ci = cr + CY[j, 0:1, :], ci + CY[j, 1:2, :]
        go = jnp.where(y > j, 1.0, 0.0).astype(F32)
        nr, ni = cmul(br, bi, wr, wi)
        wr = wr + go * (nr - wr)
        wi = wi + go * (ni - wi)
    CZ[z, 0:1, :] = cr
    CZ[z, 1:2, :] = ci
    Cr[0:1, :] = rowr
    Ci[0:1, :] = rowi
    Cr[1:2, :] = wr
    Ci[1:2, :] = wi
    for j in range(1, RING):
        carry_copy(CZ, cz_ss, cz_rs, z, (ring(z, j) * RING + y, t)).start()

    attend(1)
    wout.forward(3, 0, 6)

    carry_all(CZ, cz_ss, cz_rs).wait_recv()
    br, bi = prow[6:7, :], prow[7:8, :]
    cr = jnp.zeros((1, NST), F32)
    ci = jnp.zeros((1, NST), F32)
    for j in range(RING - 1):
        go = jnp.where(z > j, 1.0, 0.0).astype(F32)
        nr, ni = cmul(br, bi, cr, ci)
        nr, ni = nr + CZ[j, 0:1, :], ni + CZ[j, 1:2, :]
        cr = go * nr + (1.0 - go) * cr
        ci = go * ni + (1.0 - go) * ci
    cr, ci = cmul(Cr[1:2, :], Ci[1:2, :], cr, ci)
    cr, ci = cr + Cr[0:1, :], ci + Ci[0:1, :]
    for j in range(8):
        Cr[j : j + 1, :] = cr
        Ci[j : j + 1, :] = ci
        cr, ci = cmul(qr, qi, cr, ci)
        cr, ci = cr + Er[j : j + 1, :], ci + Ei[j : j + 1, :]
    cr, ci = Cr[...], Ci[...]
    for i in range(16):
        at = slice(8 * i, 8 * i + 8)
        gr, gi = cmul(pw[0, i : i + 1, :], pw[1, i : i + 1, :], cr, ci)
        Sr[at, :] = Sr[at, :] + gr
        Si[at, :] = Si[at, :] + gi
    wout.forward(3, 6, 8)
    total = up.astype(F32) * sg[...]
    for j, ref in ((0, Sr), (2, Si)):
        high, low = split(ref[...])
        total = total + nt(high, BDo[j]) + nt(low, BDo[j]) + nt(high, BDo[j + 1])
    mixed = jax.nn.gelu(total).astype(BF16)
    M[:, 256:512] = lax.dot_general(
        permute, mixed, (((0,), (0,)), ((), ())), preferred_element_type=F32
    ).astype(BF16)

    def chunk(half, a):
        wide = Wo[half, pl.ds(pl.multiple_of(a * RING, RING), RING)].reshape(256, 512)
        part = nt(M[...], wide).reshape(CHIPS, 2, 16, 256)
        at = a + RING * half
        PP[0, at] = part[:, 0]
        PP[1, at] = part[:, 1]
        return at

    def make(batch, items):
        made = [chunk(half, a) for half, a in items]
        for at in made:
            pltpu.make_async_remote_copy(
                src_ref=PP.at[1 - core, at], dst_ref=PR.at[at], send_sem=tw_ss,
                recv_sem=tw_rs.at[batch], device_id=twin, device_id_type=MESH,
            ).start()
        return made

    def twin_all(batch, count):
        ref = PR.at[pl.ds(0, count)]
        return pltpu.make_async_remote_copy(
            src_ref=ref, dst_ref=ref, send_sem=tw_ss, recv_sem=tw_rs.at[batch],
            device_id=twin, device_id_type=MESH,
        )

    def pass_on(batch, made):
        twin_all(batch, len(made)).wait_recv()
        for at in made:
            Pb[at] = (PP[core, at] + PR[at]).astype(BF16)
            R[chip, at] = Pb[at, chip]
        for at in made:
            for j in range(1, CHIPS):
                to = lax.rem(chip + j, CHIPS)
                pltpu.make_async_remote_copy(
                    src_ref=Pb.at[at, to], dst_ref=R.at[chip, at], send_sem=rs_ss,
                    recv_sem=rs_rs.at[batch], device_id=(sp, 2 * to + core), device_id_type=MESH,
                ).start()

    def owned_all(batch, count):
        ref = R.at[pl.ds(0, CHIPS - 1), pl.ds(0, count)]
        return pltpu.make_async_remote_copy(
            src_ref=ref, dst_ref=ref, send_sem=rs_ss, recv_sem=rs_rs.at[batch],
            device_id=twin, device_id_type=MESH,
        )

    def add_up(batch, made):
        owned_all(batch, len(made)).wait_recv()
        for at in made:
            total = R[0, at].astype(F32)
            for j in range(1, CHIPS):
                total = total + R[j, at].astype(F32)
            T[at] = total

    made0 = make(0, at_hop(0) + at_hop(1))
    wout.forward(4, 0, 4)
    made1 = make(1, at_hop(2))
    wout.forward(4, 4, 8)
    pass_on(0, made0)
    made2 = make(2, at_hop(3))
    pass_on(1, made1)
    pass_on(2, made2)
    wout.last()
    made3 = make(3, at_hop(4))
    pass_on(3, made3)
    add_up(0, made0)
    add_up(1, made1)
    add_up(2, made2)

    twin_all(0, 2 * RING).wait_send()
    kv_copy.wait_send()
    carry_all(CY, cy_ss, cy_rs).wait_send()
    carry_all(CZ, cz_ss, cz_rs).wait_send()
    win.drain()
    wout.drain()
    owned_all(0, 2 * RING).wait_send()
    add_up(3, made3)

    def total_square():
        square = jnp.zeros((16, 256), F32)
        for at in range(2 * RING):
            square = square + T[at] * T[at]
        return jnp.sum(square, axis=-1, keepdims=True)

    square = total_square()
    scale = lax.rsqrt(square * (1.0 / D) + EPS)
    quarter = iota((16, 128), 1) // 32
    for n in range(32):
        zz, y0 = n // 4, 2 * (n % 4)
        tile = None
        pieces = ((y0, zz), (RING + zz, y0), (y0 + 1, zz), (RING + zz, y0 + 1))
        for place, (source, at) in enumerate(pieces):
            part = T[source, :, 128 * (at // 4) : 128 * (at // 4) + 128]
            shift = (32 * place - 32 * (at % 4)) % 128
            if shift:
                part = pltpu.roll(part, shift, 1)
            tile = part if tile is None else jnp.where(quarter == place, part, tile)
        cols = slice(128 * n, 128 * n + 128)
        out_ref[:, cols] = (tile * scale * og[:, cols]).astype(BF16)


def body(
    tokens, norm_gain, w_query, w_key, w_value, w_state_in, sink_logit, decay_rate, rotation,
    log_step, in_re, in_im, out_re, out_im, skip_gain, w_attn_out, w_state_out, out_gain,
):
    vm, dma = pltpu.VMEM, pltpu.SemaphoreType.DMA
    spec = pl.BlockSpec(memory_space=pl.ANY)
    specs = [spec] * 18
    return pl.pallas_call(
        kernel,
        out_shape=jax.ShapeDtypeStruct((16, D), BF16),
        in_specs=specs,
        out_specs=pl.BlockSpec(memory_space=pltpu.VMEM),
        scratch_shapes=[
            vm((2, 64, 32, NIN), BF16),
            vm((2, 64, 32, 512), BF16),
            vm((ROWS, D), BF16),
            vm((ROWS, D), BF16),
            vm((2, RING, ROWS, 256), BF16),
            vm((64, 64), BF16),
            vm((64, 64), BF16),
            pltpu.SMEM((4,), F32),
            pltpu.SMEM((16,), F32),
            vm((1, D), F32),
            vm((1, D), F32),
            vm((1, 256), F32),
            vm((16, 64), F32),
            vm((16, 64), F32),
            vm((16, 16, 64), F32),
            vm((16, 16, 64), F32),
            vm((16, 16, 64), F32),
            vm((16, 16, 64), F32),
            vm((ROWS, NIN), F32),
            vm((ROWS, 128), F32),
            vm((ROWS, 128), F32),
            vm((8, NST), F32),
            vm((2, 16, NST), F32),
            vm((4, 256, NST), BF16),
            vm((4, 256, NST), BF16),
            vm((ROWS, NST), F32),
            vm((ROWS, NST), F32),
            vm((8, NST), F32),
            vm((8, NST), F32),
            vm((8, NST), F32),
            vm((8, NST), F32),
            vm((RING, 2, NST), F32),
            vm((RING, 2, NST), F32),
            vm((2, ROWS, 128), BF16),
            vm((ROWS, 256), BF16),
            vm((ROWS, 512), BF16),
            vm((2, 2 * RING, CHIPS, 16, 256), F32),
            vm((2 * RING, CHIPS, 16, 256), F32),
            vm((2 * RING, CHIPS, 16, 256), BF16),
            vm((CHIPS, 2 * RING, 16, 256), BF16),
            vm((2 * RING, 16, 256), F32),
            dma((22,)),
            dma, dma((2, 2, 4)), dma((2, 2, 4, RING)),
            dma, dma((2, 2, 4)), dma((2, 2, 4, RING)),
            dma, dma, dma, dma, dma, dma, dma, dma((4,)), dma, dma((4,)),
        ],
        compiler_params=pltpu.CompilerParams(collective_id=0, has_side_effects=True),
    )(
        tokens, norm_gain.reshape(1, D), w_query, w_key, w_value, w_state_in, sink_logit,
        decay_rate, rotation, log_step, in_re.transpose(0, 2, 1), in_im.transpose(0, 2, 1),
        out_re, out_im, skip_gain.reshape(1, 256), w_attn_out.T, w_state_out.T, out_gain.reshape(1, D),
    )


def solution(mesh):
    return jax.shard_map(
        body,
        mesh=mesh,
        in_specs=(
            P("sp", None),
            P(),
            P("sp", "tp"),
            P("sp", "tp"),
            P("sp", "tp"),
            P("sp", "tp"),
            P("tp"),
            P("tp", None),
            P("tp", None),
            P("tp"),
            P("tp", None, None),
            P("tp", None, None),
            P("tp", None, None),
            P("tp", None, None),
            P("tp"),
            P("tp", "sp"),
            P("tp", "sp"),
            P(),
        ),
        out_specs=P(("sp", "tp"), None),
        check_vma=False,
    )
```

```python
import math

import jax
import jax.numpy as jnp
from jax import lax
from jax.experimental import pallas as pl
from jax.experimental.pallas import tpu as pltpu
from jax.sharding import PartitionSpec as P

MESH = pl.DeviceIdType.MESH
F32 = jnp.float32
BF16 = jnp.bfloat16
EPS = 1e-06
BASE = 500000.0
RING = 8
TP = 8
CHIPS = 4
ROWS = 128
D = 4096
NQ = 384
NST = 1024
GROUPS = ((0,), (1, 2), (3, 4), (5, 6), (7,))
FLOWS = tuple((half, side) for half in (0, 1) for side in (0, 1))


ORDER = (
    ("stage", "S", 1),
    ("forward", "S", 2, 0),
    ("forward", "Q", 2, 0),
    ("stage", "Q", 1),
    ("stage", "S", 2),
    ("forward", "S", 2, 1),
    ("forward", "Q", 3, 0),
    ("stage", "Q", 2),
    ("stage", "S", 3),
    ("forward", "S", 3, 0),
    ("forward", "S", 2, 2),
    ("forward", "S", 3, 1),
    ("forward", "Q", 2, 1),
    ("norm",),
    ("stage", "S", 4),
    ("stage", "Q", 3),
    ("forward", "S", 2, 3),
    ("stage", "O", 1),
    ("forward", "S", 2, 4),
    ("stage", "Q", 4),
    ("forward", "S", 3, 2),
    ("forward", "Q", 2, 2),
    ("forward", "S", 4, 0),
    ("halves",),
    ("project", "S", 0),
    ("tables",),
    ("forward", "Q", 2, 3),
    ("forward", "S", 3, 3),
    ("project", "Q", 0),
    ("forward", "S", 3, 4),
    ("params",),
    ("forward", "Q", 2, 4),
    ("in",),
    ("forward", "Q", 3, 1),
    ("forward", "S", 4, 1),
    ("forward", "S", 4, 2),
    ("forward", "Q", 3, 2),
    ("forward", "S", 4, 3),
    ("forward", "S", 4, 4),
    ("forward", "Q", 3, 3),
    ("stage", "O", 2),
    ("forward", "Q", 3, 4),
    ("project", "Q", 1),
    ("forward", "Q", 4, 0),
    ("project", "S", 1),
    ("project", "S", 2),
    ("project", "S", 3),
    ("project", "S", 4),
    ("forward", "Q", 4, 1),
    ("forward", "Q", 4, 2),
    ("scan",),
    ("forward", "Q", 4, 3),
    ("stage", "O", 3),
    ("forward", "Q", 4, 4),
    ("forward", "O", 2, 0),
    ("forward", "O", 2, 1),
    ("stage", "O", 4),
    ("forward", "O", 2, 2),
    ("project", "Q", 2),
    ("project", "Q", 3),
    ("row",),
    ("project", "Q", 4),
    ("keys",),
    ("forward", "O", 2, 3),
    ("forward", "O", 3, 0),
    ("out",),
    ("forward", "O", 2, 4),
    ("forward", "O", 3, 1),
    ("forward", "O", 3, 2),
    ("attention",),
    ("forward", "O", 3, 3),
    ("column",),
    ("forward", "O", 3, 4),
    ("make", 0),
    ("forward", "O", 4, 0),
    ("forward", "O", 4, 1),
    ("make", 1),
    ("forward", "O", 4, 2),
    ("pass_on", 0),
    ("forward", "O", 4, 3),
    ("forward", "O", 4, 4),
    ("make", 2),
    ("pass_on", 1),
    ("pass_on", 2),
)


def nn(a, b):
    return lax.dot_general(a, b, (((1,), (0,)), ((), ())), preferred_element_type=F32)


def nt(a, b):
    return lax.dot_general(a, b, (((1,), (1,)), ((), ())), preferred_element_type=F32)


def split(x):
    high = x.astype(BF16)
    return high, (x - high.astype(F32)).astype(BF16)


def iota(shape, dim):
    return lax.broadcasted_iota(jnp.int32, shape, dim)


def ring(v, d):
    return lax.rem(v + d + 2 * RING, RING)


def cmul(ar, ai, br, bi):
    return ar * br - ai * bi, ar * bi + ai * br


def kernel(
    tok_h, ng_h, wq_h, wk_h, wv_h, ws_h, sink_h, dec_h, rot_h, ls_h,
    inre_h, inim_h, outre_h, outim_h, sg_h, wa_h, wso_h, og_h,
    out_ref,
    Ws, Wq, Wo, tok, xn, xh, kw, vw, sink_s, ls_s, ng, og, sg, dec, rot, inre, inim, outre, outim,
    us, qkv, cosr, sinr, prow, pw, BDi, BDo, Sr, Si, Er, Ei, Cr, Ci, CY, CZ, KVb, qb, M, PP, PR, Pb, R, Pl, Rl, T, upr,
    lsem, s_ssem, s_r1, s_r2, q_ssem, q_r1, q_r2, o_ssem, o_r1, o_r2, kv_ss, kv_rs, cy_ss, cy_rs, cz_ss, cz_rs,
    rs_ss, rs_rs, tw_ss, tw_rs, last_ss, last_rs,
):
    sp = lax.axis_index("sp")
    t = lax.axis_index("tp")
    z = sp // RING
    y = lax.rem(sp, RING)

    chip = t // 2
    core = lax.rem(t, 2)
    twin = (sp, t + 1 - 2 * core)
    barrier = pltpu.get_barrier_semaphore()
    after = lax.rem(sp + 1, RING * RING)
    before = lax.rem(sp + RING * RING - 1, RING * RING)
    peers = [(z * RING + ring(y, j), t) for j in range(1, RING)]
    peers += [(ring(z, j) * RING + y, t) for j in range(1, RING)]
    peers += [(sp, lax.rem(t + j, TP)) for j in range(1, TP)]
    peers += [(after, t), (before, t)]
    for peer in peers:
        pl.semaphore_signal(barrier, inc=1, device_id=peer, device_id_type=MESH)

    mine = (y * RING + z, z * RING + y)
    local = []
    for half in (0, 1):
        at = pl.ds(32 * half, 32)
        local += [
            (wq_h.at[at], Wq.at[half, mine[half], :, pl.ds(0, 256)]),
            (ws_h.at[at], Ws.at[half, mine[half]]),
        ]
    local += [
        (wk_h, kw),
        (wv_h, vw),
        (tok_h, tok),
        (ng_h, ng),
        (dec_h, dec),
        (rot_h, rot),
        (inre_h, inre),
        (inim_h, inim),
        (outre_h, outre),
        (outim_h, outim),
        (sg_h, sg),
        (og_h, og),
        (sink_h, sink_s),
        (ls_h, ls_s),
    ]
    for half in (0, 1):
        at = pl.ds(32 * half, 32)
        local += [
            (wa_h.at[at], Wo.at[half, mine[half], :, pl.ds(0, 256)]),
            (wso_h.at[at], Wo.at[half, mine[half], :, pl.ds(256, 256)]),
        ]
    copies = [pltpu.make_async_copy(a, b, lsem.at[i]) for i, (a, b) in enumerate(local)]
    for c in copies:
        c.start()

    for i in range(6):
        copies[i].wait()
    lane64 = iota((64, 128), 1)
    row64 = iota((64, 128), 0)
    to_low = (lane64 == row64).astype(F32).astype(BF16)
    to_high = (lane64 == row64 + 64).astype(F32).astype(BF16)
    kv_part = (nn(kw[...], to_low) + nn(vw[...], to_high)).astype(BF16)
    Wq[0, mine[0], :, 256:384] = kv_part[:32]
    Wq[1, mine[1], :, 256:384] = kv_part[32:]
    pl.semaphore_wait(barrier, len(peers))

    def block(half, d1, d2):
        first, second = (z, y) if half == 0 else (y, z)
        return ring(second, d2) * RING + ring(first, d1)

    def neighbour(half, phase, side):
        step = 1 if side == 0 else -1
        if (half == 0) == (phase == 1):
            return (ring(z, step) * RING + y, t)
        return (z * RING + ring(y, step), t)

    def rows(hop, side):
        return pl.ds(0, 32) if hop < 4 else pl.ds(16 * side, 16)

    def piece(buf, ssem, rsem, half, phase, hop, side, index):
        ref = buf.at[half, index, rows(hop, side)]
        return pltpu.make_async_remote_copy(
            src_ref=ref, dst_ref=ref, send_sem=ssem, recv_sem=rsem,
            device_id=neighbour(half, phase, side), device_id_type=MESH,
        )

    def sign(side):
        return 1 if side == 0 else -1

    def offset(k):
        if isinstance(k, int):
            return k // 2 if k % 2 == 0 else -((k + 1) // 2)
        return (1 - 2 * lax.rem(k, 2)) * ((k + 1) // 2)

    class Gather:
        def __init__(self, buf, ssem, r1, r2):
            self.buf, self.ssem, self.r1, self.r2 = buf, ssem, r1, r2

        def first(self, half, side, hop):
            index = block(half, -(hop - 1) * sign(side), 0)
            return piece(self.buf, self.ssem, self.r1.at[hop - 1], half, 1, hop, side, index)

        def second(self, half, side, hop, k):
            group = 15 if hop == 4 else 5 * (hop - 1) + (k + 1) // 2
            index = block(half, offset(k), -(hop - 1) * sign(side))
            return piece(self.buf, self.ssem, self.r2.at[group], half, 2, hop, side, index)

        def arrived(self, sem, count, hop):
            ref = self.buf.at[:, pl.ds(0, 2 * count), rows(hop, 0)]
            pltpu.make_async_remote_copy(
                src_ref=ref, dst_ref=ref, send_sem=self.ssem, recv_sem=sem,
                device_id=neighbour(0, 1, 0), device_id_type=MESH,
            ).wait_recv()

        def begin(self):
            for half, side in FLOWS:
                self.first(half, side, 1).start()

        def own(self, k):
            for half, side in FLOWS:
                self.second(half, side, 1, k).start()

        def stage(self, hop):
            self.arrived(self.r1.at[hop - 1], 1, hop)
            if hop < 4:
                for half, side in FLOWS:
                    self.first(half, side, hop + 1).start()
            self.own(2 * hop - 1)
            if hop < 4:
                self.own(2 * hop)

        def forward(self, hop, group):
            pieces = GROUPS[group]
            self.arrived(self.r2.at[5 * (hop - 2) + group], len(pieces), hop - 1)
            for half, side in FLOWS:
                for k in pieces:
                    self.second(half, side, hop, k).start()

        def last(self):
            self.arrived(self.r2.at[15], RING, 4)

        def drain(self):
            ref = self.buf.at[:, pl.ds(0, 63)]
            pltpu.make_async_remote_copy(
                src_ref=ref, dst_ref=ref, send_sem=self.ssem, recv_sem=self.r1.at[0],
                device_id=neighbour(0, 1, 0), device_id_type=MESH,
            ).wait_send()

    wst = Gather(Ws, s_ssem, s_r1, s_r2)
    wqk = Gather(Wq, q_ssem, q_r1, q_r2)
    wout = Gather(Wo, o_ssem, o_r1, o_r2)

    for i in (18, 19, 20, 21):
        copies[i].wait()
    for gather in (wst, wqk, wout):
        gather.begin()
        gather.own(0)

    lane_full = iota((ROWS, 128), 1)
    low_half = lax.rem(lane_full, 64) < 32
    spread64 = (lax.rem(iota((64, NST), 1), 64) == iota((64, NST), 0)).astype(F32)
    permute = (
        iota((ROWS, ROWS), 1)
        == 16 * lax.rem(iota((ROWS, ROWS), 0), 8) + iota((ROWS, ROWS), 0) // 8
    ).astype(F32).astype(BF16)
    def carry_copy(buf, ss, rs, at, peer):
        return pltpu.make_async_remote_copy(
            src_ref=buf.at[at], dst_ref=buf.at[at], send_sem=ss, recv_sem=rs,
            device_id=peer, device_id_type=MESH,
        )

    def carry_all(buf, ss, rs):
        return carry_copy(buf, ss, rs, pl.ds(0, 7), peers[0])

    kv_copy = pltpu.make_async_remote_copy(
        src_ref=KVb.at[1], dst_ref=KVb.at[0], send_sem=kv_ss, recv_sem=kv_rs,
        device_id=(after, t), device_id_type=MESH,
    )
    def swapped(x):
        return jnp.where(low_half, pltpu.roll(x, 96, 1), pltpu.roll(x, 32, 1))

    spread64b = spread64.astype(BF16)
    own_block = iota((256, NST), 0) // 16 == iota((256, NST), 1) // 64

    def diagonal(dst, at, value):
        for part, value in enumerate(split(value.reshape(256, 64))):
            dst[at + part] = jnp.where(own_block, nn(value, spread64b), 0.0).astype(BF16)

    def norm():
        copies[6].wait()
        copies[7].wait()

        def norm_step(i, c):
            at = pl.ds(pl.multiple_of(i * 16, 16), 16)
            x = tok[at, :].astype(F32)
            scale = lax.rsqrt(jnp.mean(x * x, axis=-1, keepdims=True) + EPS)
            xn[at, :] = (x * scale * ng[...]).astype(BF16)
            return c

        lax.fori_loop(0, ROWS // 16, norm_step, 0)

    def halves():
        lane128 = iota((ROWS, 128), 1) // 32
        source = iota((512, 256), 0)
        target = iota((512, 256), 1)
        spot = 64 * (target // 32) + lax.rem(target, 32)
        picks = [(source == spot + 32 * half).astype(F32).astype(BF16) for half in (0, 1)]
        for i in range(RING):
            xh[1, i] = nn(xn[:, 512 * i : 512 * i + 512], picks[1]).astype(BF16)
        for group in range(2):
            rolled = []
            for i in range(4):
                at = 512 * (4 * group + i)
                part = nn(xn[:, at : at + 512], picks[0])
                rolled.append((part[:, :128], part[:, 128:]))
            for j in range(RING):
                tile = None
                for i in range(4):
                    part = rolled[i][j // 4]
                    shift = 32 * ((i - j) % 4)
                    if shift:
                        part = pltpu.roll(part, shift, 1)
                    tile = part if tile is None else jnp.where(lane128 == i, part, tile)
                xh[0, j, :, 128 * group : 128 * group + 128] = tile.astype(BF16)


    def tables():
        lane = iota((1, 128), 1)
        freq = jnp.zeros((1, 128), F32)
        for i in range(32):
            freq = jnp.where(lax.rem(lane, 32) == i, F32(BASE ** (-2.0 * i / 64)), freq)
        position = (sp * ROWS + iota((ROWS, 128), 0)).astype(F32)
        angle = position * freq
        cosr[...] = jnp.cos(angle)
        sine = jnp.sin(angle)
        sinr[...] = jnp.where(low_half, -sine, sine)

    def params():
        for i in (8, 9, 17):
            copies[i].wait()
        lane_n = iota((1, NST), 1)
        own_group = iota((16, NST), 1) // 64 == iota((16, NST), 0)

        def as_row(ref):
            tiled = lax.dot_general(
                ref[...], spread64, (((1,), (0,)), ((), ())),
                precision=lax.Precision.HIGHEST, preferred_element_type=F32,
            )
            return jnp.sum(jnp.where(own_group, tiled, 0.0), axis=0, keepdims=True)

        lam_re = -as_row(dec)
        lam_im = as_row(rot)
        step_log = jnp.zeros((1, NST), F32)
        for g in range(16):
            step_log = jnp.where(lane_n // 64 == g, ls_s[g], step_log)
        delta = jnp.exp(step_log)
        modulus = jnp.exp(lam_re * delta)
        pr = modulus * jnp.cos(lam_im * delta)
        pi = modulus * jnp.sin(lam_im * delta)
        less = pr - 1.0
        den = lam_re * lam_re + lam_im * lam_im
        prow[0:1, :] = (less * lam_re + pi * lam_im) / den
        prow[1:2, :] = (pi * lam_re - less * lam_im) / den
        ar, ai = pr, pi
        for k in range(16):
            pw[0, k : k + 1, :] = ar
            pw[1, k : k + 1, :] = ai
            if k < 15:
                ar, ai = cmul(ar, ai, pr, pi)
        prow[2:3, :] = ar
        prow[3:4, :] = ai
        for _ in range(3):
            ar, ai = cmul(ar, ai, ar, ai)
        prow[4:5, :] = ar
        prow[5:6, :] = ai
        for _ in range(3):
            ar, ai = cmul(ar, ai, ar, ai)
        prow[6:7, :] = ar
        prow[7:8, :] = ai

    def diag_in():
        for i in (10, 11, 12, 13):
            copies[i].wait()
        diagonal(BDi, 0, inre[...])
        diagonal(BDi, 2, inim[...])

    def diag_out():
        diagonal(BDo, 0, outre[...])
        diagonal(BDo, 2, -outim[...])
        for i in (14, 15, 16):
            copies[i].wait()

    def at_hop(hop):
        if hop == 0:
            return [(0, y), (1, z)]
        if hop == 4:
            return [(0, ring(y, 4)), (1, ring(z, 4))]
        return [(0, ring(y, hop)), (0, ring(y, -hop)), (1, ring(z, hop)), (1, ring(z, -hop))]

    def projects(weights, out, hop):
        for n, (half, a) in enumerate(at_hop(hop)):
            wide = weights[half, pl.ds(pl.multiple_of(a * RING, RING), RING)]
            part = nn(xh[half, a], wide.reshape(256, out.shape[1]))
            out[...] = part if hop == 0 and n == 0 else out[...] + part

    def scan():
        u = us[...].astype(BF16)
        up = nn(permute, u).astype(BF16)
        upr[...] = up
        Sr[...] = nn(up, BDi[0]) + nn(up, BDi[1])
        Si[...] = nn(up, BDi[2]) + nn(up, BDi[3])
        fr, fi = prow[0:1, :], prow[1:2, :]
        pr, pi = pw[0, 0:1, :], pw[1, 0:1, :]
        sr = jnp.zeros((8, NST), F32)
        si = jnp.zeros((8, NST), F32)
        for i in range(16):
            at = slice(8 * i, 8 * i + 8)
            br, bi = cmul(fr, fi, Sr[at, :], Si[at, :])
            sr, si = cmul(pr, pi, sr, si)
            sr, si = sr + br, si + bi
            Sr[at, :] = sr
            Si[at, :] = si
        Er[...] = sr
        Ei[...] = si
        qr, qi = prow[2:3, :], prow[3:4, :]
        cr = jnp.zeros((1, NST), F32)
        ci = jnp.zeros((1, NST), F32)
        for j in range(8):
            cr, ci = cmul(qr, qi, cr, ci)
            cr, ci = cr + Er[j : j + 1, :], ci + Ei[j : j + 1, :]
        CY[y, 0:1, :] = cr
        CY[y, 1:2, :] = ci

        for j in range(1, RING):
            carry_copy(CY, cy_ss, cy_rs, y, (z * RING + ring(y, j), t)).start()

    def carry_row():
        carry_all(CY, cy_ss, cy_rs).wait_recv()
        br, bi = prow[4:5, :], prow[5:6, :]
        cr = jnp.zeros((1, NST), F32)
        ci = jnp.zeros((1, NST), F32)
        rowr, rowi = cr, ci
        wr, wi = cr + 1.0, ci
        for j in range(RING):
            keep = jnp.where(y == j, 1.0, 0.0).astype(F32)
            rowr = rowr + keep * cr
            rowi = rowi + keep * ci
            cr, ci = cmul(br, bi, cr, ci)
            cr, ci = cr + CY[j, 0:1, :], ci + CY[j, 1:2, :]
            go = jnp.where(y > j, 1.0, 0.0).astype(F32)
            nr, ni = cmul(br, bi, wr, wi)
            wr = wr + go * (nr - wr)
            wi = wi + go * (ni - wi)
        CZ[z, 0:1, :] = cr
        CZ[z, 1:2, :] = ci
        Cr[0:1, :] = rowr
        Ci[0:1, :] = rowi
        Cr[1:2, :] = wr
        Ci[1:2, :] = wi
        for j in range(1, RING):
            carry_copy(CZ, cz_ss, cz_rs, z, (ring(z, j) * RING + y, t)).start()


    def carry_column():
        qr, qi = prow[2:3, :], prow[3:4, :]
        carry_all(CZ, cz_ss, cz_rs).wait_recv()
        br, bi = prow[6:7, :], prow[7:8, :]
        cr = jnp.zeros((1, NST), F32)
        ci = jnp.zeros((1, NST), F32)
        for j in range(RING - 1):
            go = jnp.where(z > j, 1.0, 0.0).astype(F32)
            nr, ni = cmul(br, bi, cr, ci)
            nr, ni = nr + CZ[j, 0:1, :], ni + CZ[j, 1:2, :]
            cr = go * nr + (1.0 - go) * cr
            ci = go * ni + (1.0 - go) * ci
        cr, ci = cmul(Cr[1:2, :], Ci[1:2, :], cr, ci)
        cr, ci = cr + Cr[0:1, :], ci + Ci[0:1, :]
        for j in range(8):
            Cr[j : j + 1, :] = cr
            Ci[j : j + 1, :] = ci
            cr, ci = cmul(qr, qi, cr, ci)
            cr, ci = cr + Er[j : j + 1, :], ci + Ei[j : j + 1, :]
        cr, ci = Cr[...], Ci[...]
        for i in range(16):
            at = slice(8 * i, 8 * i + 8)
            gr, gi = cmul(pw[0, i : i + 1, :], pw[1, i : i + 1, :], cr, ci)
            Sr[at, :] = Sr[at, :] + gr
            Si[at, :] = Si[at, :] + gi
        total = upr[...].astype(F32) * sg[...]
        for j, ref in ((0, Sr), (2, Si)):
            high, low = split(ref[...])
            total = total + nt(high, BDo[j]) + nt(low, BDo[j])
        mixed = jax.nn.gelu(total).astype(BF16)
        M[:, 256:512] = lax.dot_general(
            permute, mixed, (((0,), (0,)), ((), ())), preferred_element_type=F32
        ).astype(BF16)


    def keys():
        kv = qkv[:, 256:384]
        key_lane = lane_full < 64
        kv = kv * jnp.where(key_lane, cosr[...], 1.0) + swapped(kv) * jnp.where(
            key_lane, sinr[...], 0.0
        )
        KVb[1] = kv.astype(BF16)
        kv_copy.start()

        for pair in range(2):
            x = qkv[:, 128 * pair : 128 * pair + 128]
            qb[:, 128 * pair : 128 * pair + 128] = (x * cosr[...] + swapped(x) * sinr[...]).astype(BF16)

    def attention():
        kv_copy.wait_recv()
        both = KVb[...].reshape(2 * ROWS, 128).astype(F32)
        turned = pltpu.roll(both, 64, 1)
        first_half = iota((2 * ROWS, 128), 1) < 64
        k_low = jnp.where(first_half, both, 0.0).astype(BF16)
        k_high = jnp.where(first_half, 0.0, turned).astype(BF16)
        v_low = jnp.where(first_half, turned, 0.0).astype(BF16)
        v_high = jnp.where(first_half, 0.0, both).astype(BF16)
        gap = iota((ROWS, 2 * ROWS), 0) + ROWS - iota((ROWS, 2 * ROWS), 1)
        key_at = sp * ROWS - ROWS + iota((ROWS, 2 * ROWS), 1)
        visible = (gap >= 0) & (gap < ROWS) & (key_at >= 0)

        def attend(pair):
            q = qb[:, 128 * pair : 128 * pair + 128]
            total = None
            for side, (k, v) in enumerate(((k_low, v_low), (k_high, v_high))):
                score = jnp.where(visible, nt(q, k) * 0.125, -jnp.inf)
                sink = sink_s[2 * pair + side]
                top = jnp.maximum(jnp.max(score, axis=-1, keepdims=True), sink)
                e = jnp.exp(score - top)
                weight = e / (jnp.sum(e, axis=-1, keepdims=True) + jnp.exp(sink - top))
                part = nn(weight.astype(BF16), v)
                total = part if total is None else total + part
            M[:, 128 * pair : 128 * pair + 128] = total.astype(BF16)


        attend(0)
        attend(1)

    def chunk(half, a, slot=None):
        wide = Wo[half, pl.ds(pl.multiple_of(a * RING, RING), RING)].reshape(256, 512)
        part = nt(M[...], wide)
        at = a + RING * half
        if slot is not None:
            Pl[slot] = part.astype(BF16).reshape(TP, 16, 256)
            Rl[t, slot] = Pl[slot, t]
            return at
        part = part.reshape(CHIPS, 2, 16, 256)
        PP[0, at] = part[:, 0]
        PP[1, at] = part[:, 1]
        return at

    def make(batch, items):
        made = [chunk(half, a) for half, a in items]
        for at in made:
            pltpu.make_async_remote_copy(
                src_ref=PP.at[1 - core, at], dst_ref=PR.at[at], send_sem=tw_ss,
                recv_sem=tw_rs.at[batch], device_id=twin, device_id_type=MESH,
            ).start()
        return made

    def twin_all(batch, count):
        ref = PR.at[pl.ds(0, count)]
        return pltpu.make_async_remote_copy(
            src_ref=ref, dst_ref=ref, send_sem=tw_ss, recv_sem=tw_rs.at[batch],
            device_id=twin, device_id_type=MESH,
        )

    def pass_on(batch, made):
        twin_all(batch, len(made)).wait_recv()
        for at in made:
            Pb[at] = (PP[core, at] + PR[at]).astype(BF16)
            R[chip, at] = Pb[at, chip]
        for at in made:
            for j in range(1, CHIPS):
                to = lax.rem(chip + j, CHIPS)
                pltpu.make_async_remote_copy(
                    src_ref=Pb.at[at, to], dst_ref=R.at[chip, at], send_sem=rs_ss,
                    recv_sem=rs_rs.at[batch], device_id=(sp, 2 * to + core), device_id_type=MESH,
                ).start()

    def owned_all(batch, count):
        ref = R.at[pl.ds(0, CHIPS - 1), pl.ds(0, count)]
        return pltpu.make_async_remote_copy(
            src_ref=ref, dst_ref=ref, send_sem=rs_ss, recv_sem=rs_rs.at[batch],
            device_id=twin, device_id_type=MESH,
        )

    def add_up(batch, made):
        owned_all(batch, len(made)).wait_recv()
        for at in made:
            total = R[0, at].astype(F32)
            for j in range(1, CHIPS):
                total = total + R[j, at].astype(F32)
            T[at] = total

    def make_last():
        made = [chunk(half, a, slot) for slot, (half, a) in enumerate(at_hop(4))]
        for slot in range(2):
            for j in range(1, TP):
                to = lax.rem(t + j, TP)
                pltpu.make_async_remote_copy(
                    src_ref=Pl.at[slot, to], dst_ref=Rl.at[t, slot], send_sem=last_ss,
                    recv_sem=last_rs, device_id=(sp, to), device_id_type=MESH,
                ).start()
        return made

    def last_all():
        ref = Rl.at[pl.ds(0, TP - 1)]
        return pltpu.make_async_remote_copy(
            src_ref=ref, dst_ref=ref, send_sem=last_ss, recv_sem=last_rs,
            device_id=twin, device_id_type=MESH,
        )

    gathers = {"S": wst, "Q": wqk, "O": wout}
    outs = {"S": (Ws, us), "Q": (Wq, qkv)}
    calls = {
        "norm": norm, "halves": halves, "tables": tables, "params": params, "in": diag_in,
        "out": diag_out, "scan": scan, "row": carry_row, "column": carry_column, "keys": keys,
        "attention": attention,
    }
    made = {}
    for name, *where in ORDER:
        if name == "stage":
            gathers[where[0]].stage(where[1])
        elif name == "forward":
            gathers[where[0]].forward(where[1], where[2])
        elif name == "project":
            if where[1] == 4:
                gathers[where[0]].last()
            projects(*outs[where[0]], where[1])
        elif name == "make":
            batch = where[0]
            made[batch] = make(batch, at_hop(0) + at_hop(1) if batch == 0 else at_hop(batch + 1))
        elif name == "pass_on":
            pass_on(where[0], made[where[0]])
        else:
            calls[name]()
    wout.last()
    made3 = make_last()
    for batch in range(3):
        add_up(batch, made[batch])

    twin_all(0, 14).wait_send()
    kv_copy.wait_send()
    carry_all(CY, cy_ss, cy_rs).wait_send()
    carry_all(CZ, cz_ss, cz_rs).wait_send()
    wst.drain()
    wqk.drain()
    wout.drain()
    owned_all(0, 14).wait_send()
    last_all().wait_send()
    last_all().wait_recv()
    for slot, at in enumerate(made3):
        total = Rl[0, slot].astype(F32)
        for j in range(1, TP):
            total = total + Rl[j, slot].astype(F32)
        T[at] = total

    def total_square():
        square = jnp.zeros((16, 256), F32)
        for at in range(2 * RING):
            square = square + T[at] * T[at]
        return jnp.sum(square, axis=-1, keepdims=True)

    square = total_square()
    scale = lax.rsqrt(square * (1.0 / D) + EPS)
    quarter = iota((16, 128), 1) // 32
    for n in range(32):
        zz, y0 = n // 4, 2 * (n % 4)
        tile = None
        pieces = ((y0, zz), (RING + zz, y0), (y0 + 1, zz), (RING + zz, y0 + 1))
        for place, (source, at) in enumerate(pieces):
            part = T[source, :, 128 * (at // 4) : 128 * (at // 4) + 128]
            shift = (32 * place - 32 * (at % 4)) % 128
            if shift:
                part = pltpu.roll(part, shift, 1)
            tile = part if tile is None else jnp.where(quarter == place, part, tile)
        cols = slice(128 * n, 128 * n + 128)
        out_ref[:, cols] = (tile * scale * og[:, cols]).astype(BF16)


def body(
    tokens, norm_gain, w_query, w_key, w_value, w_state_in, sink_logit, decay_rate, rotation,
    log_step, in_re, in_im, out_re, out_im, skip_gain, w_attn_out, w_state_out, out_gain,
):
    vm, dma = pltpu.VMEM, pltpu.SemaphoreType.DMA
    spec = pl.BlockSpec(memory_space=pl.ANY)
    specs = [spec] * 18
    return pl.pallas_call(
        kernel,
        out_shape=jax.ShapeDtypeStruct((16, D), BF16),
        in_specs=specs,
        out_specs=pl.BlockSpec(memory_space=pltpu.VMEM),
        scratch_shapes=[
            vm((2, 64, 32, 256), BF16),
            vm((2, 64, 32, NQ), BF16),
            vm((2, 64, 32, 512), BF16),
            vm((ROWS, D), BF16),
            vm((ROWS, D), BF16),
            vm((2, RING, ROWS, 256), BF16),
            vm((64, 64), BF16),
            vm((64, 64), BF16),
            pltpu.SMEM((4,), F32),
            pltpu.SMEM((16,), F32),
            vm((1, D), F32),
            vm((1, D), F32),
            vm((1, 256), F32),
            vm((16, 64), F32),
            vm((16, 64), F32),
            vm((16, 16, 64), F32),
            vm((16, 16, 64), F32),
            vm((16, 16, 64), F32),
            vm((16, 16, 64), F32),
            vm((ROWS, 256), F32),
            vm((ROWS, NQ), F32),
            vm((ROWS, 128), F32),
            vm((ROWS, 128), F32),
            vm((8, NST), F32),
            vm((2, 16, NST), F32),
            vm((4, 256, NST), BF16),
            vm((4, 256, NST), BF16),
            vm((ROWS, NST), F32),
            vm((ROWS, NST), F32),
            vm((8, NST), F32),
            vm((8, NST), F32),
            vm((8, NST), F32),
            vm((8, NST), F32),
            vm((RING, 2, NST), F32),
            vm((RING, 2, NST), F32),
            vm((2, ROWS, 128), BF16),
            vm((ROWS, 256), BF16),
            vm((ROWS, 512), BF16),
            vm((2, 2 * RING, CHIPS, 16, 256), F32),
            vm((2 * RING, CHIPS, 16, 256), F32),
            vm((2 * RING, CHIPS, 16, 256), BF16),
            vm((CHIPS, 2 * RING, 16, 256), BF16),
            vm((2, TP, 16, 256), BF16),
            vm((TP, 2, 16, 256), BF16),
            vm((2 * RING, 16, 256), F32),
            vm((ROWS, 256), BF16),
            dma((22,)),
            dma, dma((4,)), dma((16,)),
            dma, dma((4,)), dma((16,)),
            dma, dma((4,)), dma((16,)),
            dma, dma, dma, dma, dma, dma, dma, dma((3,)), dma, dma((3,)), dma, dma,
        ],
        compiler_params=pltpu.CompilerParams(collective_id=0, has_side_effects=True),
    )(
        tokens, norm_gain.reshape(1, D), w_query, w_key, w_value, w_state_in, sink_logit,
        decay_rate, rotation, log_step, in_re.transpose(0, 2, 1), in_im.transpose(0, 2, 1),
        out_re, out_im, skip_gain.reshape(1, 256), w_attn_out.T, w_state_out.T, out_gain.reshape(1, D),
    )


def solution(mesh):
    return jax.shard_map(
        body,
        mesh=mesh,
        in_specs=(
            P("sp", None),
            P(),
            P("sp", "tp"),
            P("sp", "tp"),
            P("sp", "tp"),
            P("sp", "tp"),
            P("tp"),
            P("tp", None),
            P("tp", None),
            P("tp"),
            P("tp", None, None),
            P("tp", None, None),
            P("tp", None, None),
            P("tp", None, None),
            P("tp"),
            P("tp", "sp"),
            P("tp", "sp"),
            P(),
        ),
        out_specs=P(("sp", "tp"), None),
        check_vma=False,
    )
```

```python
import math

import jax
import jax.numpy as jnp
from jax import lax
from jax.experimental import pallas as pl
from jax.experimental.pallas import tpu as pltpu
from jax.sharding import PartitionSpec as P

MESH = pl.DeviceIdType.MESH
F32 = jnp.float32
BF16 = jnp.bfloat16
EPS = 1e-06
BASE = 500000.0
RING = 8
TP = 8
CHIPS = 4
ROWS = 128
D = 4096
NQ = 384
NST = 1024
GROUPS = ((0,), (1, 2), (3, 4), (5, 6), (7,))
FLOWS = tuple((half, side) for half in (0, 1) for side in (0, 1))


ORDER = (
    ("stage", "S", 1),
    ("forward", "S", 2, 0),
    ("forward", "Q", 2, 0),
    ("stage", "Q", 1),
    ("stage", "S", 2),
    ("forward", "S", 2, 1),
    ("forward", "Q", 3, 0),
    ("stage", "Q", 2),
    ("stage", "S", 3),
    ("forward", "S", 3, 0),
    ("forward", "S", 2, 2),
    ("forward", "S", 3, 1),
    ("forward", "Q", 2, 1),
    ("norm",),
    ("stage", "S", 4),
    ("stage", "Q", 3),
    ("forward", "S", 2, 3),
    ("stage", "O", 1),
    ("forward", "S", 2, 4),
    ("stage", "Q", 4),
    ("forward", "S", 3, 2),
    ("forward", "Q", 2, 2),
    ("forward", "S", 4, 0),
    ("halves",),
    ("project", "S", 0),
    ("tables",),
    ("forward", "Q", 2, 3),
    ("forward", "S", 3, 3),
    ("project", "Q", 0),
    ("forward", "S", 3, 4),
    ("params",),
    ("forward", "Q", 2, 4),
    ("in",),
    ("forward", "Q", 3, 1),
    ("forward", "S", 4, 1),
    ("forward", "S", 4, 2),
    ("forward", "Q", 3, 2),
    ("forward", "S", 4, 3),
    ("forward", "S", 4, 4),
    ("forward", "Q", 3, 3),
    ("stage", "O", 2),
    ("forward", "Q", 3, 4),
    ("project", "Q", 1),
    ("forward", "Q", 4, 0),
    ("project", "S", 1),
    ("project", "S", 2),
    ("project", "S", 3),
    ("project", "S", 4),
    ("forward", "Q", 4, 1),
    ("forward", "Q", 4, 2),
    ("scan",),
    ("forward", "Q", 4, 3),
    ("stage", "O", 3),
    ("forward", "Q", 4, 4),
    ("forward", "O", 2, 0),
    ("forward", "O", 2, 1),
    ("stage", "O", 4),
    ("forward", "O", 2, 2),
    ("project", "Q", 2),
    ("project", "Q", 3),
    ("row",),
    ("project", "Q", 4),
    ("keys",),
    ("forward", "O", 2, 3),
    ("forward", "O", 3, 0),
    ("out",),
    ("forward", "O", 2, 4),
    ("forward", "O", 3, 1),
    ("forward", "O", 3, 2),
    ("attention",),
    ("forward", "O", 3, 3),
    ("column",),
    ("forward", "O", 3, 4),
    ("make", 0),
    ("forward", "O", 4, 0),
    ("forward", "O", 4, 1),
    ("make", 1),
    ("forward", "O", 4, 2),
    ("pass_on", 0),
    ("forward", "O", 4, 3),
    ("forward", "O", 4, 4),
    ("make", 2),
    ("pass_on", 1),
    ("pass_on", 2),
)


def nn(a, b):
    return lax.dot_general(a, b, (((1,), (0,)), ((), ())), preferred_element_type=F32)


def nt(a, b):
    return lax.dot_general(a, b, (((1,), (1,)), ((), ())), preferred_element_type=F32)


def split(x):
    high = x.astype(BF16)
    return high, (x - high.astype(F32)).astype(BF16)


def iota(shape, dim):
    return lax.broadcasted_iota(jnp.int32, shape, dim)


def ring(v, d):
    return lax.rem(v + d + 2 * RING, RING)


def cmul(ar, ai, br, bi):
    return ar * br - ai * bi, ar * bi + ai * br


def kernel(
    tok_h, ng_h, wq_h, wk_h, wv_h, ws_h, sink_h, dec_h, rot_h, ls_h,
    inre_h, inim_h, outre_h, outim_h, sg_h, wa_h, wso_h, og_h,
    out_ref,
    Ws, Wq, Wo, tok, xn, xh, kw, vw, sink_s, ls_s, ng, og, sg, dec, rot, inre, inim, outre, outim,
    us, qkv, cosr, sinr, prow, pw, BDi, BDo, Sr, Si, Er, Ei, Cr, Ci, CY, CZ, KVb, qb, M, PP, PR, Pb, R, Pl, Rl, T, upr,
    lsem, s_ssem, s_r1, s_r2, q_ssem, q_r1, q_r2, o_ssem, o_r1, o_r2, kv_ss, kv_rs, cy_ss, cy_rs, cz_ss, cz_rs,
    rs_ss, rs_rs, tw_ss, tw_rs, last_ss, last_rs,
):
    sp = lax.axis_index("sp")
    t = lax.axis_index("tp")
    z = sp // RING
    y = lax.rem(sp, RING)

    chip = t // 2
    core = lax.rem(t, 2)
    twin = (sp, t + 1 - 2 * core)
    barrier = pltpu.get_barrier_semaphore()
    after = lax.rem(sp + 1, RING * RING)
    before = lax.rem(sp + RING * RING - 1, RING * RING)
    peers = [(z * RING + ring(y, j), t) for j in range(1, RING)]
    peers += [(ring(z, j) * RING + y, t) for j in range(1, RING)]
    peers += [(sp, lax.rem(t + j, TP)) for j in range(1, TP)]
    peers += [(after, t), (before, t)]
    for peer in peers:
        pl.semaphore_signal(barrier, inc=1, device_id=peer, device_id_type=MESH)

    mine = (y * RING + z, z * RING + y)
    local = []
    for half in (0, 1):
        at = pl.ds(32 * half, 32)
        local += [
            (wq_h.at[at], Wq.at[half, mine[half], :, pl.ds(0, 256)]),
            (ws_h.at[at], Ws.at[half, mine[half]]),
        ]
    local += [
        (wk_h, kw),
        (wv_h, vw),
        (tok_h, tok),
        (ng_h, ng),
        (dec_h, dec),
        (rot_h, rot),
        (inre_h, inre),
        (inim_h, inim),
        (outre_h, outre),
        (outim_h, outim),
        (sg_h, sg),
        (og_h, og),
        (sink_h, sink_s),
        (ls_h, ls_s),
    ]
    for half in (0, 1):
        at = pl.ds(32 * half, 32)
        local += [
            (wa_h.at[at], Wo.at[half, mine[half], :, pl.ds(0, 256)]),
            (wso_h.at[at], Wo.at[half, mine[half], :, pl.ds(256, 256)]),
        ]
    copies = [pltpu.make_async_copy(a, b, lsem.at[i]) for i, (a, b) in enumerate(local)]
    for c in copies:
        c.start()

    for i in (1, 3):
        copies[i].wait()
    pl.semaphore_wait(barrier, len(peers))

    def block(half, d1, d2):
        first, second = (z, y) if half == 0 else (y, z)
        return ring(second, d2) * RING + ring(first, d1)

    def neighbour(half, phase, side):
        step = 1 if side == 0 else -1
        if (half == 0) == (phase == 1):
            return (ring(z, step) * RING + y, t)
        return (z * RING + ring(y, step), t)

    def rows(hop, side):
        return pl.ds(0, 32) if hop < 4 else pl.ds(16 * side, 16)

    def piece(buf, ssem, rsem, half, phase, hop, side, index):
        ref = buf.at[half, index, rows(hop, side)]
        return pltpu.make_async_remote_copy(
            src_ref=ref, dst_ref=ref, send_sem=ssem, recv_sem=rsem,
            device_id=neighbour(half, phase, side), device_id_type=MESH,
        )

    def sign(side):
        return 1 if side == 0 else -1

    def offset(k):
        if isinstance(k, int):
            return k // 2 if k % 2 == 0 else -((k + 1) // 2)
        return (1 - 2 * lax.rem(k, 2)) * ((k + 1) // 2)

    class Gather:
        def __init__(self, buf, ssem, r1, r2):
            self.buf, self.ssem, self.r1, self.r2 = buf, ssem, r1, r2

        def first(self, half, side, hop):
            index = block(half, -(hop - 1) * sign(side), 0)
            return piece(self.buf, self.ssem, self.r1.at[hop - 1], half, 1, hop, side, index)

        def second(self, half, side, hop, k):
            group = 15 if hop == 4 else 5 * (hop - 1) + (k + 1) // 2
            index = block(half, offset(k), -(hop - 1) * sign(side))
            return piece(self.buf, self.ssem, self.r2.at[group], half, 2, hop, side, index)

        def arrived(self, sem, count, hop):
            ref = self.buf.at[:, pl.ds(0, 2 * count), rows(hop, 0)]
            pltpu.make_async_remote_copy(
                src_ref=ref, dst_ref=ref, send_sem=self.ssem, recv_sem=sem,
                device_id=neighbour(0, 1, 0), device_id_type=MESH,
            ).wait_recv()

        def begin(self):
            for half, side in FLOWS:
                self.first(half, side, 1).start()

        def own(self, k):
            for half, side in FLOWS:
                self.second(half, side, 1, k).start()

        def stage(self, hop):
            self.arrived(self.r1.at[hop - 1], 1, hop)
            if hop < 4:
                for half, side in FLOWS:
                    self.first(half, side, hop + 1).start()
            self.own(2 * hop - 1)
            if hop < 4:
                self.own(2 * hop)

        def forward(self, hop, group):
            pieces = GROUPS[group]
            self.arrived(self.r2.at[5 * (hop - 2) + group], len(pieces), hop - 1)
            for half, side in FLOWS:
                for k in pieces:
                    self.second(half, side, hop, k).start()

        def last(self):
            self.arrived(self.r2.at[15], RING, 4)

        def drain(self):
            ref = self.buf.at[:, pl.ds(0, 63)]
            pltpu.make_async_remote_copy(
                src_ref=ref, dst_ref=ref, send_sem=self.ssem, recv_sem=self.r1.at[0],
                device_id=neighbour(0, 1, 0), device_id_type=MESH,
            ).wait_send()

    wst = Gather(Ws, s_ssem, s_r1, s_r2)
    wqk = Gather(Wq, q_ssem, q_r1, q_r2)
    wout = Gather(Wo, o_ssem, o_r1, o_r2)

    wst.begin()
    wst.own(0)
    for i in (0, 2, 4, 5):
        copies[i].wait()
    lane64 = iota((64, 128), 1)
    row64 = iota((64, 128), 0)
    to_low = (lane64 == row64).astype(F32).astype(BF16)
    to_high = (lane64 == row64 + 64).astype(F32).astype(BF16)
    kv_part = (nn(kw[...], to_low) + nn(vw[...], to_high)).astype(BF16)
    Wq[0, mine[0], :, 256:384] = kv_part[:32]
    Wq[1, mine[1], :, 256:384] = kv_part[32:]
    for i in (18, 19, 20, 21):
        copies[i].wait()
    for gather in (wqk, wout):
        gather.begin()
        gather.own(0)

    lane_full = iota((ROWS, 128), 1)
    low_half = lax.rem(lane_full, 64) < 32
    spread64 = (lax.rem(iota((64, NST), 1), 64) == iota((64, NST), 0)).astype(F32)
    permute = (
        iota((ROWS, ROWS), 1)
        == 16 * lax.rem(iota((ROWS, ROWS), 0), 8) + iota((ROWS, ROWS), 0) // 8
    ).astype(F32).astype(BF16)
    def carry_copy(buf, ss, rs, at, peer):
        return pltpu.make_async_remote_copy(
            src_ref=buf.at[at], dst_ref=buf.at[at], send_sem=ss, recv_sem=rs,
            device_id=peer, device_id_type=MESH,
        )

    def carry_all(buf, ss, rs):
        return carry_copy(buf, ss, rs, pl.ds(0, 7), peers[0])

    kv_copy = pltpu.make_async_remote_copy(
        src_ref=KVb.at[1], dst_ref=KVb.at[0], send_sem=kv_ss, recv_sem=kv_rs,
        device_id=(after, t), device_id_type=MESH,
    )
    def swapped(x):
        return jnp.where(low_half, pltpu.roll(x, 96, 1), pltpu.roll(x, 32, 1))

    spread64b = spread64.astype(BF16)
    own_block = iota((256, NST), 0) // 16 == iota((256, NST), 1) // 64

    def diagonal(dst, at, value):
        for part, value in enumerate(split(value.reshape(256, 64))):
            dst[at + part] = jnp.where(own_block, nn(value, spread64b), 0.0).astype(BF16)

    def norm():
        copies[6].wait()
        copies[7].wait()

        def norm_step(i, c):
            at = pl.ds(pl.multiple_of(i * 16, 16), 16)
            x = tok[at, :].astype(F32)
            scale = lax.rsqrt(jnp.mean(x * x, axis=-1, keepdims=True) + EPS)
            xn[at, :] = (x * scale * ng[...]).astype(BF16)
            return c

        lax.fori_loop(0, ROWS // 16, norm_step, 0)

    def halves():
        lane128 = iota((ROWS, 128), 1) // 32
        source = iota((512, 256), 0)
        target = iota((512, 256), 1)
        spot = 64 * (target // 32) + lax.rem(target, 32)
        picks = [(source == spot + 32 * half).astype(F32).astype(BF16) for half in (0, 1)]
        for i in range(RING):
            xh[1, i] = nn(xn[:, 512 * i : 512 * i + 512], picks[1]).astype(BF16)
        for group in range(2):
            rolled = []
            for i in range(4):
                at = 512 * (4 * group + i)
                part = nn(xn[:, at : at + 512], picks[0])
                rolled.append((part[:, :128], part[:, 128:]))
            for j in range(RING):
                tile = None
                for i in range(4):
                    part = rolled[i][j // 4]
                    shift = 32 * ((i - j) % 4)
                    if shift:
                        part = pltpu.roll(part, shift, 1)
                    tile = part if tile is None else jnp.where(lane128 == i, part, tile)
                xh[0, j, :, 128 * group : 128 * group + 128] = tile.astype(BF16)


    def tables():
        lane = iota((1, 128), 1)
        freq = jnp.zeros((1, 128), F32)
        for i in range(32):
            freq = jnp.where(lax.rem(lane, 32) == i, F32(BASE ** (-2.0 * i / 64)), freq)
        position = (sp * ROWS + iota((ROWS, 128), 0)).astype(F32)
        angle = position * freq
        cosr[...] = jnp.cos(angle)
        sine = jnp.sin(angle)
        sinr[...] = jnp.where(low_half, -sine, sine)

    def params():
        for i in (8, 9, 17):
            copies[i].wait()
        lane_n = iota((1, NST), 1)
        own_group = iota((16, NST), 1) // 64 == iota((16, NST), 0)

        def as_row(ref):
            tiled = lax.dot_general(
                ref[...], spread64, (((1,), (0,)), ((), ())),
                precision=lax.Precision.HIGHEST, preferred_element_type=F32,
            )
            return jnp.sum(jnp.where(own_group, tiled, 0.0), axis=0, keepdims=True)

        lam_re = -as_row(dec)
        lam_im = as_row(rot)
        step_log = jnp.zeros((1, NST), F32)
        for g in range(16):
            step_log = jnp.where(lane_n // 64 == g, ls_s[g], step_log)
        delta = jnp.exp(step_log)
        modulus = jnp.exp(lam_re * delta)
        pr = modulus * jnp.cos(lam_im * delta)
        pi = modulus * jnp.sin(lam_im * delta)
        less = pr - 1.0
        den = lam_re * lam_re + lam_im * lam_im
        prow[0:1, :] = (less * lam_re + pi * lam_im) / den
        prow[1:2, :] = (pi * lam_re - less * lam_im) / den
        ar, ai = pr, pi
        for k in range(16):
            pw[0, k : k + 1, :] = ar
            pw[1, k : k + 1, :] = ai
            if k < 15:
                ar, ai = cmul(ar, ai, pr, pi)
        prow[2:3, :] = ar
        prow[3:4, :] = ai
        for _ in range(3):
            ar, ai = cmul(ar, ai, ar, ai)
        prow[4:5, :] = ar
        prow[5:6, :] = ai
        for _ in range(3):
            ar, ai = cmul(ar, ai, ar, ai)
        prow[6:7, :] = ar
        prow[7:8, :] = ai

    def diag_in():
        for i in (10, 11, 12, 13):
            copies[i].wait()
        diagonal(BDi, 0, inre[...])
        diagonal(BDi, 2, inim[...])

    def diag_out():
        diagonal(BDo, 0, outre[...])
        diagonal(BDo, 2, -outim[...])
        for i in (14, 15, 16):
            copies[i].wait()

    def at_hop(hop):
        if hop == 0:
            return [(0, y), (1, z)]
        if hop == 4:
            return [(0, ring(y, 4)), (1, ring(z, 4))]
        return [(0, ring(y, hop)), (0, ring(y, -hop)), (1, ring(z, hop)), (1, ring(z, -hop))]

    def projects(weights, out, hop):
        for n, (half, a) in enumerate(at_hop(hop)):
            wide = weights[half, pl.ds(pl.multiple_of(a * RING, RING), RING)]
            part = nn(xh[half, a], wide.reshape(256, out.shape[1]))
            out[...] = part if hop == 0 and n == 0 else out[...] + part

    def scan():
        u = us[...].astype(BF16)
        up = nn(permute, u).astype(BF16)
        upr[...] = up
        Sr[...] = nn(up, BDi[0]) + nn(up, BDi[1])
        Si[...] = nn(up, BDi[2]) + nn(up, BDi[3])
        fr, fi = prow[0:1, :], prow[1:2, :]
        pr, pi = pw[0, 0:1, :], pw[1, 0:1, :]
        sr = jnp.zeros((8, NST), F32)
        si = jnp.zeros((8, NST), F32)
        for i in range(16):
            at = slice(8 * i, 8 * i + 8)
            br, bi = cmul(fr, fi, Sr[at, :], Si[at, :])
            sr, si = cmul(pr, pi, sr, si)
            sr, si = sr + br, si + bi
            Sr[at, :] = sr
            Si[at, :] = si
        Er[...] = sr
        Ei[...] = si
        qr, qi = prow[2:3, :], prow[3:4, :]
        cr = jnp.zeros((1, NST), F32)
        ci = jnp.zeros((1, NST), F32)
        for j in range(8):
            cr, ci = cmul(qr, qi, cr, ci)
            cr, ci = cr + Er[j : j + 1, :], ci + Ei[j : j + 1, :]
        CY[y, 0:1, :] = cr
        CY[y, 1:2, :] = ci

        for j in range(1, RING):
            carry_copy(CY, cy_ss, cy_rs, y, (z * RING + ring(y, j), t)).start()

    def carry_row():
        carry_all(CY, cy_ss, cy_rs).wait_recv()
        br, bi = prow[4:5, :], prow[5:6, :]
        cr = jnp.zeros((1, NST), F32)
        ci = jnp.zeros((1, NST), F32)
        rowr, rowi = cr, ci
        wr, wi = cr + 1.0, ci
        for j in range(RING):
            keep = jnp.where(y == j, 1.0, 0.0).astype(F32)
            rowr = rowr + keep * cr
            rowi = rowi + keep * ci
            cr, ci = cmul(br, bi, cr, ci)
            cr, ci = cr + CY[j, 0:1, :], ci + CY[j, 1:2, :]
            go = jnp.where(y > j, 1.0, 0.0).astype(F32)
            nr, ni = cmul(br, bi, wr, wi)
            wr = wr + go * (nr - wr)
            wi = wi + go * (ni - wi)
        CZ[z, 0:1, :] = cr
        CZ[z, 1:2, :] = ci
        Cr[0:1, :] = rowr
        Ci[0:1, :] = rowi
        Cr[1:2, :] = wr
        Ci[1:2, :] = wi
        for j in range(1, RING):
            carry_copy(CZ, cz_ss, cz_rs, z, (ring(z, j) * RING + y, t)).start()


    def carry_column():
        qr, qi = prow[2:3, :], prow[3:4, :]
        carry_all(CZ, cz_ss, cz_rs).wait_recv()
        br, bi = prow[6:7, :], prow[7:8, :]
        cr = jnp.zeros((1, NST), F32)
        ci = jnp.zeros((1, NST), F32)
        for j in range(RING - 1):
            go = jnp.where(z > j, 1.0, 0.0).astype(F32)
            nr, ni = cmul(br, bi, cr, ci)
            nr, ni = nr + CZ[j, 0:1, :], ni + CZ[j, 1:2, :]
            cr = go * nr + (1.0 - go) * cr
            ci = go * ni + (1.0 - go) * ci
        cr, ci = cmul(Cr[1:2, :], Ci[1:2, :], cr, ci)
        cr, ci = cr + Cr[0:1, :], ci + Ci[0:1, :]
        for j in range(8):
            Cr[j : j + 1, :] = cr
            Ci[j : j + 1, :] = ci
            cr, ci = cmul(qr, qi, cr, ci)
            cr, ci = cr + Er[j : j + 1, :], ci + Ei[j : j + 1, :]
        cr, ci = Cr[...], Ci[...]
        for i in range(16):
            at = slice(8 * i, 8 * i + 8)
            gr, gi = cmul(pw[0, i : i + 1, :], pw[1, i : i + 1, :], cr, ci)
            Sr[at, :] = Sr[at, :] + gr
            Si[at, :] = Si[at, :] + gi
        total = upr[...].astype(F32) * sg[...]
        for j, ref in ((0, Sr), (2, Si)):
            high, low = split(ref[...])
            total = total + nt(high, BDo[j]) + nt(low, BDo[j])
        mixed = jax.nn.gelu(total).astype(BF16)
        M[:, 256:512] = lax.dot_general(
            permute, mixed, (((0,), (0,)), ((), ())), preferred_element_type=F32
        ).astype(BF16)


    def keys():
        kv = qkv[:, 256:384]
        key_lane = lane_full < 64
        kv = kv * jnp.where(key_lane, cosr[...], 1.0) + swapped(kv) * jnp.where(
            key_lane, sinr[...], 0.0
        )
        KVb[1] = kv.astype(BF16)
        kv_copy.start()

        for pair in range(2):
            x = qkv[:, 128 * pair : 128 * pair + 128]
            qb[:, 128 * pair : 128 * pair + 128] = (x * cosr[...] + swapped(x) * sinr[...]).astype(BF16)

    def attention():
        kv_copy.wait_recv()
        both = KVb[...].reshape(2 * ROWS, 128).astype(F32)
        turned = pltpu.roll(both, 64, 1)
        first_half = iota((2 * ROWS, 128), 1) < 64
        k_low = jnp.where(first_half, both, 0.0).astype(BF16)
        k_high = jnp.where(first_half, 0.0, turned).astype(BF16)
        v_low = jnp.where(first_half, turned, 0.0).astype(BF16)
        v_high = jnp.where(first_half, 0.0, both).astype(BF16)
        gap = iota((ROWS, 2 * ROWS), 0) + ROWS - iota((ROWS, 2 * ROWS), 1)
        key_at = sp * ROWS - ROWS + iota((ROWS, 2 * ROWS), 1)
        visible = (gap >= 0) & (gap < ROWS) & (key_at >= 0)

        def attend(pair):
            q = qb[:, 128 * pair : 128 * pair + 128]
            total = None
            for side, (k, v) in enumerate(((k_low, v_low), (k_high, v_high))):
                score = jnp.where(visible, nt(q, k) * 0.125, -jnp.inf)
                sink = sink_s[2 * pair + side]
                top = jnp.maximum(jnp.max(score, axis=-1, keepdims=True), sink)
                e = jnp.exp(score - top)
                weight = e / (jnp.sum(e, axis=-1, keepdims=True) + jnp.exp(sink - top))
                part = nn(weight.astype(BF16), v)
                total = part if total is None else total + part
            M[:, 128 * pair : 128 * pair + 128] = total.astype(BF16)


        attend(0)
        attend(1)

    def chunk(half, a, slot=None):
        wide = Wo[half, pl.ds(pl.multiple_of(a * RING, RING), RING)].reshape(256, 512)
        part = nt(M[...], wide)
        at = a + RING * half
        if slot is not None:
            Pl[slot] = part.astype(BF16).reshape(TP, 16, 256)
            Rl[t, slot] = Pl[slot, t]
            return at
        part = part.reshape(CHIPS, 2, 16, 256)
        PP[0, at] = part[:, 0]
        PP[1, at] = part[:, 1]
        return at

    def make(batch, items):
        made = [chunk(half, a) for half, a in items]
        for at in made:
            pltpu.make_async_remote_copy(
                src_ref=PP.at[1 - core, at], dst_ref=PR.at[at], send_sem=tw_ss,
                recv_sem=tw_rs.at[batch], device_id=twin, device_id_type=MESH,
            ).start()
        return made

    def twin_all(batch, count):
        ref = PR.at[pl.ds(0, count)]
        return pltpu.make_async_remote_copy(
            src_ref=ref, dst_ref=ref, send_sem=tw_ss, recv_sem=tw_rs.at[batch],
            device_id=twin, device_id_type=MESH,
        )

    def pass_on(batch, made):
        twin_all(batch, len(made)).wait_recv()
        for at in made:
            Pb[at] = (PP[core, at] + PR[at]).astype(BF16)
            R[chip, at] = Pb[at, chip]
        for at in made:
            for j in (2, 1, 3):
                to = lax.rem(chip + j, CHIPS)
                pltpu.make_async_remote_copy(
                    src_ref=Pb.at[at, to], dst_ref=R.at[chip, at], send_sem=rs_ss,
                    recv_sem=rs_rs.at[batch], device_id=(sp, 2 * to + core), device_id_type=MESH,
                ).start()

    def owned_all(batch, count):
        ref = R.at[pl.ds(0, CHIPS - 1), pl.ds(0, count)]
        return pltpu.make_async_remote_copy(
            src_ref=ref, dst_ref=ref, send_sem=rs_ss, recv_sem=rs_rs.at[batch],
            device_id=twin, device_id_type=MESH,
        )

    def add_up(batch, made):
        owned_all(batch, len(made)).wait_recv()
        for at in made:
            total = R[0, at].astype(F32)
            for j in range(1, CHIPS):
                total = total + R[j, at].astype(F32)
            T[at] = total

    def make_last():
        made = [chunk(half, a, slot) for slot, (half, a) in enumerate(at_hop(4))]
        for slot in range(2):
            for j in (4, 5, 2, 3, 6, 7, 1):
                to = 2 * lax.rem(chip + j // 2, CHIPS) + lax.rem(core + j, 2)
                pltpu.make_async_remote_copy(
                    src_ref=Pl.at[slot, to], dst_ref=Rl.at[t, slot], send_sem=last_ss,
                    recv_sem=last_rs, device_id=(sp, to), device_id_type=MESH,
                ).start()
        return made

    def last_all():
        ref = Rl.at[pl.ds(0, TP - 1)]
        return pltpu.make_async_remote_copy(
            src_ref=ref, dst_ref=ref, send_sem=last_ss, recv_sem=last_rs,
            device_id=twin, device_id_type=MESH,
        )

    gathers = {"S": wst, "Q": wqk, "O": wout}
    outs = {"S": (Ws, us), "Q": (Wq, qkv)}
    calls = {
        "norm": norm, "halves": halves, "tables": tables, "params": params, "in": diag_in,
        "out": diag_out, "scan": scan, "row": carry_row, "column": carry_column, "keys": keys,
        "attention": attention,
    }
    made = {}
    for name, *where in ORDER:
        if name == "stage":
            gathers[where[0]].stage(where[1])
        elif name == "forward":
            gathers[where[0]].forward(where[1], where[2])
        elif name == "project":
            if where[1] == 4:
                gathers[where[0]].last()
            projects(*outs[where[0]], where[1])
        elif name == "make":
            batch = where[0]
            made[batch] = make(batch, at_hop(0) + at_hop(1) if batch == 0 else at_hop(batch + 1))
        elif name == "pass_on":
            pass_on(where[0], made[where[0]])
        else:
            calls[name]()
    wout.last()
    made3 = make_last()
    for batch in range(3):
        add_up(batch, made[batch])

    twin_all(0, 14).wait_send()
    kv_copy.wait_send()
    carry_all(CY, cy_ss, cy_rs).wait_send()
    carry_all(CZ, cz_ss, cz_rs).wait_send()
    wst.drain()
    wqk.drain()
    wout.drain()
    owned_all(0, 14).wait_send()
    last_all().wait_send()
    last_all().wait_recv()
    for slot, at in enumerate(made3):
        total = Rl[0, slot].astype(F32)
        for j in range(1, TP):
            total = total + Rl[j, slot].astype(F32)
        T[at] = total

    def total_square():
        square = jnp.zeros((16, 256), F32)
        for at in range(2 * RING):
            square = square + T[at] * T[at]
        return jnp.sum(square, axis=-1, keepdims=True)

    square = total_square()
    scale = lax.rsqrt(square * (1.0 / D) + EPS)
    quarter = iota((16, 128), 1) // 32
    for n in range(32):
        zz, y0 = n // 4, 2 * (n % 4)
        tile = None
        pieces = ((y0, zz), (RING + zz, y0), (y0 + 1, zz), (RING + zz, y0 + 1))
        for place, (source, at) in enumerate(pieces):
            part = T[source, :, 128 * (at // 4) : 128 * (at // 4) + 128]
            shift = (32 * place - 32 * (at % 4)) % 128
            if shift:
                part = pltpu.roll(part, shift, 1)
            tile = part if tile is None else jnp.where(quarter == place, part, tile)
        cols = slice(128 * n, 128 * n + 128)
        out_ref[:, cols] = (tile * scale * og[:, cols]).astype(BF16)


def body(
    tokens, norm_gain, w_query, w_key, w_value, w_state_in, sink_logit, decay_rate, rotation,
    log_step, in_re, in_im, out_re, out_im, skip_gain, w_attn_out, w_state_out, out_gain,
):
    vm, dma = pltpu.VMEM, pltpu.SemaphoreType.DMA
    spec = pl.BlockSpec(memory_space=pl.ANY)
    specs = [spec] * 18
    return pl.pallas_call(
        kernel,
        out_shape=pltpu.VMEM((16, D), BF16),
        in_specs=specs,
        out_specs=pl.BlockSpec(memory_space=pltpu.VMEM),
        scratch_shapes=[
            vm((2, 64, 32, 256), BF16),
            vm((2, 64, 32, NQ), BF16),
            vm((2, 64, 32, 512), BF16),
            vm((ROWS, D), BF16),
            vm((ROWS, D), BF16),
            vm((2, RING, ROWS, 256), BF16),
            vm((64, 64), BF16),
            vm((64, 64), BF16),
            pltpu.SMEM((4,), F32),
            pltpu.SMEM((16,), F32),
            vm((1, D), F32),
            vm((1, D), F32),
            vm((1, 256), F32),
            vm((16, 64), F32),
            vm((16, 64), F32),
            vm((16, 16, 64), F32),
            vm((16, 16, 64), F32),
            vm((16, 16, 64), F32),
            vm((16, 16, 64), F32),
            vm((ROWS, 256), F32),
            vm((ROWS, NQ), F32),
            vm((ROWS, 128), F32),
            vm((ROWS, 128), F32),
            vm((8, NST), F32),
            vm((2, 16, NST), F32),
            vm((4, 256, NST), BF16),
            vm((4, 256, NST), BF16),
            vm((ROWS, NST), F32),
            vm((ROWS, NST), F32),
            vm((8, NST), F32),
            vm((8, NST), F32),
            vm((8, NST), F32),
            vm((8, NST), F32),
            vm((RING, 2, NST), F32),
            vm((RING, 2, NST), F32),
            vm((2, ROWS, 128), BF16),
            vm((ROWS, 256), BF16),
            vm((ROWS, 512), BF16),
            vm((2, 2 * RING, CHIPS, 16, 256), F32),
            vm((2 * RING, CHIPS, 16, 256), F32),
            vm((2 * RING, CHIPS, 16, 256), BF16),
            vm((CHIPS, 2 * RING, 16, 256), BF16),
            vm((2, TP, 16, 256), BF16),
            vm((TP, 2, 16, 256), BF16),
            vm((2 * RING, 16, 256), F32),
            vm((ROWS, 256), BF16),
            dma((22,)),
            dma, dma((4,)), dma((16,)),
            dma, dma((4,)), dma((16,)),
            dma, dma((4,)), dma((16,)),
            dma, dma, dma, dma, dma, dma, dma, dma((3,)), dma, dma((3,)), dma, dma,
        ],
        compiler_params=pltpu.CompilerParams(collective_id=0, has_side_effects=True),
    )(
        tokens, norm_gain.reshape(1, D), w_query, w_key, w_value, w_state_in, sink_logit,
        decay_rate, rotation, log_step, in_re.transpose(0, 2, 1), in_im.transpose(0, 2, 1),
        out_re, out_im, skip_gain.reshape(1, 256), w_attn_out.T, w_state_out.T, out_gain.reshape(1, D),
    )


def solution(mesh):
    return jax.shard_map(
        body,
        mesh=mesh,
        in_specs=(
            P("sp", None),
            P(),
            P("sp", "tp"),
            P("sp", "tp"),
            P("sp", "tp"),
            P("sp", "tp"),
            P("tp"),
            P("tp", None),
            P("tp", None),
            P("tp"),
            P("tp", None, None),
            P("tp", None, None),
            P("tp", None, None),
            P("tp", None, None),
            P("tp"),
            P("tp", "sp"),
            P("tp", "sp"),
            P(),
        ),
        out_specs=P(("sp", "tp"), None),
        check_vma=False,
    )
```

```python
import math

import jax
import jax.numpy as jnp
from jax import lax
from jax.experimental import pallas as pl
from jax.experimental.pallas import tpu as pltpu
from jax.sharding import PartitionSpec as P

MESH = pl.DeviceIdType.MESH
F32 = jnp.float32
BF16 = jnp.bfloat16
EPS = 1e-06
BASE = 500000.0
RING = 8
TP = 8
CHIPS = 4
ROWS = 128
D = 4096
NQ = 384
NST = 1024
GROUPS = ((0,), (1, 2), (3, 4), (5, 6), (7,))
FLOWS = tuple((half, side) for half in (0, 1) for side in (0, 1))


ORDER = (
    ("stage", "S", 1),
    ("forward", "S", 2, 0),
    ("forward", "Q", 2, 0),
    ("stage", "Q", 1),
    ("stage", "S", 2),
    ("forward", "S", 2, 1),
    ("forward", "Q", 3, 0),
    ("stage", "Q", 2),
    ("stage", "S", 3),
    ("forward", "S", 3, 0),
    ("forward", "S", 2, 2),
    ("forward", "S", 3, 1),
    ("forward", "Q", 2, 1),
    ("norm",),
    ("stage", "S", 4),
    ("stage", "Q", 3),
    ("forward", "S", 2, 3),
    ("stage", "O", 1),
    ("forward", "S", 2, 4),
    ("stage", "Q", 4),
    ("forward", "S", 3, 2),
    ("forward", "Q", 2, 2),
    ("forward", "S", 4, 0),
    ("halves",),
    ("project", "S", 0),
    ("tables",),
    ("forward", "Q", 2, 3),
    ("forward", "S", 3, 3),
    ("project", "Q", 0),
    ("forward", "S", 3, 4),
    ("params",),
    ("forward", "Q", 2, 4),
    ("in",),
    ("forward", "Q", 3, 1),
    ("forward", "S", 4, 1),
    ("forward", "S", 4, 2),
    ("forward", "Q", 3, 2),
    ("forward", "S", 4, 3),
    ("forward", "S", 4, 4),
    ("forward", "Q", 3, 3),
    ("stage", "O", 2),
    ("forward", "Q", 3, 4),
    ("project", "Q", 1),
    ("forward", "Q", 4, 0),
    ("project", "S", 1),
    ("project", "S", 2),
    ("project", "S", 3),
    ("project", "S", 4),
    ("forward", "Q", 4, 1),
    ("forward", "Q", 4, 2),
    ("scan",),
    ("forward", "Q", 4, 3),
    ("stage", "O", 3),
    ("forward", "Q", 4, 4),
    ("forward", "O", 2, 0),
    ("forward", "O", 2, 1),
    ("stage", "O", 4),
    ("forward", "O", 2, 2),
    ("project", "Q", 2),
    ("project", "Q", 3),
    ("row",),
    ("project", "Q", 4),
    ("keys",),
    ("forward", "O", 2, 3),
    ("forward", "O", 3, 0),
    ("out",),
    ("forward", "O", 2, 4),
    ("forward", "O", 3, 1),
    ("forward", "O", 3, 2),
    ("attention",),
    ("forward", "O", 3, 3),
    ("column",),
    ("forward", "O", 3, 4),
    ("make", 0),
    ("forward", "O", 4, 0),
    ("forward", "O", 4, 1),
    ("make", 1),
    ("forward", "O", 4, 2),
    ("pass_on", 0),
    ("forward", "O", 4, 3),
    ("forward", "O", 4, 4),
    ("make", 2),
    ("pass_on", 1),
    ("pass_on", 2),
)


def nn(a, b):
    return lax.dot_general(a, b, (((1,), (0,)), ((), ())), preferred_element_type=F32)


def nt(a, b):
    return lax.dot_general(a, b, (((1,), (1,)), ((), ())), preferred_element_type=F32)


def split(x):
    high = x.astype(BF16)
    return high, (x - high.astype(F32)).astype(BF16)


def iota(shape, dim):
    return lax.broadcasted_iota(jnp.int32, shape, dim)


def ring(v, d):
    return lax.rem(v + d + 2 * RING, RING)


def cmul(ar, ai, br, bi):
    return ar * br - ai * bi, ar * bi + ai * br


def kernel(
    tok_h, ng_h, wq_h, wk_h, wv_h, ws_h, sink_s, dec_h, rot_h, ls_s,
    inre_h, inim_h, outre_h, outim_h, sg_h, wa_h, wso_h, og_h,
    out_ref,
    Ws, Wq, Wo, tok, xn, xh, kw, vw, ng, og, sg, dec, rot, inre, inim, outre, outim,
    us, qkv, cosr, sinr, prow, pw, BDi, BDo, Sr, Si, Er, Ei, Cr, Ci, CY, CZ, KVb, qb, M, PP, PR, Pb, R, Pl, Rl, T, upr,
    lsem, s_ssem, s_r1, s_r2, q_ssem, q_r1, q_r2, o_ssem, o_r1, o_r2, kv_ss, kv_rs, cy_ss, cy_rs, cz_ss, cz_rs,
    rs_ss, rs_rs, tw_ss, tw_rs, last_ss, last_rs,
):
    sp = lax.axis_index("sp")
    t = lax.axis_index("tp")
    z = sp // RING
    y = lax.rem(sp, RING)

    chip = t // 2
    core = lax.rem(t, 2)
    twin = (sp, t + 1 - 2 * core)
    barrier = pltpu.get_barrier_semaphore()
    after = lax.rem(sp + 1, RING * RING)
    before = lax.rem(sp + RING * RING - 1, RING * RING)
    peers = [(z * RING + ring(y, j), t) for j in range(1, RING)]
    peers += [(ring(z, j) * RING + y, t) for j in range(1, RING)]
    peers += [(sp, lax.rem(t + j, TP)) for j in range(1, TP)]
    peers += [(after, t), (before, t)]
    for peer in peers:
        pl.semaphore_signal(barrier, inc=1, device_id=peer, device_id_type=MESH)

    mine = (y * RING + z, z * RING + y)
    local = []
    for half in (0, 1):
        at = pl.ds(32 * half, 32)
        local += [
            (wq_h.at[at], Wq.at[half, mine[half], :, pl.ds(0, 256)]),
            (ws_h.at[at], Ws.at[half, mine[half]]),
        ]
    local += [
        (wk_h, kw),
        (wv_h, vw),
        (tok_h, tok),
        (ng_h, ng),
        (dec_h, dec),
        (rot_h, rot),
        (inre_h, inre),
        (inim_h, inim),
        (outre_h, outre),
        (outim_h, outim),
        (sg_h, sg),
        (og_h, og),
    ]
    for half in (0, 1):
        at = pl.ds(32 * half, 32)
        local += [
            (wa_h.at[at], Wo.at[half, mine[half], :, pl.ds(0, 256)]),
            (wso_h.at[at], Wo.at[half, mine[half], :, pl.ds(256, 256)]),
        ]
    copies = [pltpu.make_async_copy(a, b, lsem.at[i]) for i, (a, b) in enumerate(local)]
    for c in copies:
        c.start()

    for i in (1, 3):
        copies[i].wait()
    pl.semaphore_wait(barrier, len(peers))

    def block(half, d1, d2):
        first, second = (z, y) if half == 0 else (y, z)
        return ring(second, d2) * RING + ring(first, d1)

    def neighbour(half, phase, side):
        step = 1 if side == 0 else -1
        if (half == 0) == (phase == 1):
            return (ring(z, step) * RING + y, t)
        return (z * RING + ring(y, step), t)

    def rows(hop, side):
        return pl.ds(0, 32) if hop < 4 else pl.ds(16 * side, 16)

    def piece(buf, ssem, rsem, half, phase, hop, side, index):
        ref = buf.at[half, index, rows(hop, side)]
        return pltpu.make_async_remote_copy(
            src_ref=ref, dst_ref=ref, send_sem=ssem, recv_sem=rsem,
            device_id=neighbour(half, phase, side), device_id_type=MESH,
        )

    def sign(side):
        return 1 if side == 0 else -1

    def offset(k):
        if isinstance(k, int):
            return k // 2 if k % 2 == 0 else -((k + 1) // 2)
        return (1 - 2 * lax.rem(k, 2)) * ((k + 1) // 2)

    class Gather:
        def __init__(self, buf, ssem, r1, r2):
            self.buf, self.ssem, self.r1, self.r2 = buf, ssem, r1, r2

        def first(self, half, side, hop):
            index = block(half, -(hop - 1) * sign(side), 0)
            return piece(self.buf, self.ssem, self.r1.at[hop - 1], half, 1, hop, side, index)

        def second(self, half, side, hop, k):
            group = 15 if hop == 4 else 5 * (hop - 1) + (k + 1) // 2
            index = block(half, offset(k), -(hop - 1) * sign(side))
            return piece(self.buf, self.ssem, self.r2.at[group], half, 2, hop, side, index)

        def arrived(self, sem, count, hop):
            ref = self.buf.at[:, pl.ds(0, 2 * count), rows(hop, 0)]
            pltpu.make_async_remote_copy(
                src_ref=ref, dst_ref=ref, send_sem=self.ssem, recv_sem=sem,
                device_id=neighbour(0, 1, 0), device_id_type=MESH,
            ).wait_recv()

        def begin(self):
            for half, side in FLOWS:
                self.first(half, side, 1).start()

        def own(self, k):
            for half, side in FLOWS:
                self.second(half, side, 1, k).start()

        def stage(self, hop):
            self.arrived(self.r1.at[hop - 1], 1, hop)
            if hop < 4:
                for half, side in FLOWS:
                    self.first(half, side, hop + 1).start()
            self.own(2 * hop - 1)
            if hop < 4:
                self.own(2 * hop)

        def forward(self, hop, group):
            pieces = GROUPS[group]
            self.arrived(self.r2.at[5 * (hop - 2) + group], len(pieces), hop - 1)
            for half, side in FLOWS:
                for k in pieces:
                    self.second(half, side, hop, k).start()

        def last(self):
            self.arrived(self.r2.at[15], RING, 4)

        def drain(self):
            ref = self.buf.at[:, pl.ds(0, 63)]
            pltpu.make_async_remote_copy(
                src_ref=ref, dst_ref=ref, send_sem=self.ssem, recv_sem=self.r1.at[0],
                device_id=neighbour(0, 1, 0), device_id_type=MESH,
            ).wait_send()

    wst = Gather(Ws, s_ssem, s_r1, s_r2)
    wqk = Gather(Wq, q_ssem, q_r1, q_r2)
    wout = Gather(Wo, o_ssem, o_r1, o_r2)

    wst.begin()
    wst.own(0)
    for i in (0, 2, 4, 5):
        copies[i].wait()
    lane64 = iota((64, 128), 1)
    row64 = iota((64, 128), 0)
    to_low = (lane64 == row64).astype(F32).astype(BF16)
    to_high = (lane64 == row64 + 64).astype(F32).astype(BF16)
    kv_part = (nn(kw[...], to_low) + nn(vw[...], to_high)).astype(BF16)
    Wq[0, mine[0], :, 256:384] = kv_part[:32]
    Wq[1, mine[1], :, 256:384] = kv_part[32:]
    for i in (16, 17, 18, 19):
        copies[i].wait()
    for gather in (wqk, wout):
        gather.begin()
        gather.own(0)

    lane_full = iota((ROWS, 128), 1)
    low_half = lax.rem(lane_full, 64) < 32
    spread64 = (lax.rem(iota((64, NST), 1), 64) == iota((64, NST), 0)).astype(F32)
    permute = (
        iota((ROWS, ROWS), 1)
        == 16 * lax.rem(iota((ROWS, ROWS), 0), 8) + iota((ROWS, ROWS), 0) // 8
    ).astype(F32).astype(BF16)
    def carry_copy(buf, ss, rs, at, peer):
        return pltpu.make_async_remote_copy(
            src_ref=buf.at[at], dst_ref=buf.at[at], send_sem=ss, recv_sem=rs,
            device_id=peer, device_id_type=MESH,
        )

    def carry_all(buf, ss, rs):
        return carry_copy(buf, ss, rs, pl.ds(0, 7), peers[0])

    kv_copy = pltpu.make_async_remote_copy(
        src_ref=KVb.at[1], dst_ref=KVb.at[0], send_sem=kv_ss, recv_sem=kv_rs,
        device_id=(after, t), device_id_type=MESH,
    )
    def swapped(x):
        return jnp.where(low_half, pltpu.roll(x, 96, 1), pltpu.roll(x, 32, 1))

    spread64b = spread64.astype(BF16)
    own_block = iota((256, NST), 0) // 16 == iota((256, NST), 1) // 64

    def diagonal(dst, at, value):
        for part, value in enumerate(split(value.reshape(256, 64))):
            dst[at + part] = jnp.where(own_block, nn(value, spread64b), 0.0).astype(BF16)

    def norm():
        copies[6].wait()
        copies[7].wait()

        def norm_step(i, c):
            at = pl.ds(pl.multiple_of(i * 16, 16), 16)
            x = tok[at, :].astype(F32)
            scale = lax.rsqrt(jnp.mean(x * x, axis=-1, keepdims=True) + EPS)
            xn[at, :] = (x * scale * ng[...]).astype(BF16)
            return c

        lax.fori_loop(0, ROWS // 16, norm_step, 0)

    def halves():
        lane128 = iota((ROWS, 128), 1) // 32
        source = iota((512, 256), 0)
        target = iota((512, 256), 1)
        spot = 64 * (target // 32) + lax.rem(target, 32)
        picks = [(source == spot + 32 * half).astype(F32).astype(BF16) for half in (0, 1)]
        for i in range(RING):
            xh[1, i] = nn(xn[:, 512 * i : 512 * i + 512], picks[1]).astype(BF16)
        for group in range(2):
            rolled = []
            for i in range(4):
                at = 512 * (4 * group + i)
                part = nn(xn[:, at : at + 512], picks[0])
                rolled.append((part[:, :128], part[:, 128:]))
            for j in range(RING):
                tile = None
                for i in range(4):
                    part = rolled[i][j // 4]
                    shift = 32 * ((i - j) % 4)
                    if shift:
                        part = pltpu.roll(part, shift, 1)
                    tile = part if tile is None else jnp.where(lane128 == i, part, tile)
                xh[0, j, :, 128 * group : 128 * group + 128] = tile.astype(BF16)


    def tables():
        lane = iota((1, 128), 1)
        freq = jnp.zeros((1, 128), F32)
        for i in range(32):
            freq = jnp.where(lax.rem(lane, 32) == i, F32(BASE ** (-2.0 * i / 64)), freq)
        position = (sp * ROWS + iota((ROWS, 128), 0)).astype(F32)
        angle = position * freq
        cosr[...] = jnp.cos(angle)
        sine = jnp.sin(angle)
        sinr[...] = jnp.where(low_half, -sine, sine)

    def params():
        for i in (8, 9):
            copies[i].wait()
        lane_n = iota((1, NST), 1)
        own_group = iota((16, NST), 1) // 64 == iota((16, NST), 0)

        def as_row(ref):
            tiled = lax.dot_general(
                ref[...], spread64, (((1,), (0,)), ((), ())),
                precision=lax.Precision.HIGHEST, preferred_element_type=F32,
            )
            return jnp.sum(jnp.where(own_group, tiled, 0.0), axis=0, keepdims=True)

        lam_re = -as_row(dec)
        lam_im = as_row(rot)
        step_log = jnp.zeros((1, NST), F32)
        for g in range(16):
            step_log = jnp.where(lane_n // 64 == g, ls_s[g], step_log)
        delta = jnp.exp(step_log)
        modulus = jnp.exp(lam_re * delta)
        pr = modulus * jnp.cos(lam_im * delta)
        pi = modulus * jnp.sin(lam_im * delta)
        less = pr - 1.0
        den = lam_re * lam_re + lam_im * lam_im
        prow[0:1, :] = (less * lam_re + pi * lam_im) / den
        prow[1:2, :] = (pi * lam_re - less * lam_im) / den
        ar, ai = pr, pi
        for k in range(16):
            pw[0, k : k + 1, :] = ar
            pw[1, k : k + 1, :] = ai
            if k < 15:
                ar, ai = cmul(ar, ai, pr, pi)
        prow[2:3, :] = ar
        prow[3:4, :] = ai
        for _ in range(3):
            ar, ai = cmul(ar, ai, ar, ai)
        prow[4:5, :] = ar
        prow[5:6, :] = ai
        for _ in range(3):
            ar, ai = cmul(ar, ai, ar, ai)
        prow[6:7, :] = ar
        prow[7:8, :] = ai

    def diag_in():
        for i in (10, 11, 12, 13):
            copies[i].wait()
        diagonal(BDi, 0, inre[...])
        diagonal(BDi, 2, inim[...])

    def diag_out():
        diagonal(BDo, 0, outre[...])
        diagonal(BDo, 2, -outim[...])
        for i in (14, 15):
            copies[i].wait()

    def at_hop(hop):
        if hop == 0:
            return [(0, y), (1, z)]
        if hop == 4:
            return [(0, ring(y, 4)), (1, ring(z, 4))]
        return [(0, ring(y, hop)), (0, ring(y, -hop)), (1, ring(z, hop)), (1, ring(z, -hop))]

    def projects(weights, out, hop):
        for n, (half, a) in enumerate(at_hop(hop)):
            wide = weights[half, pl.ds(pl.multiple_of(a * RING, RING), RING)]
            part = nn(xh[half, a], wide.reshape(256, out.shape[1]))
            out[...] = part if hop == 0 and n == 0 else out[...] + part

    def scan():
        u = us[...].astype(BF16)
        up = nn(permute, u).astype(BF16)
        upr[...] = up
        Sr[...] = nn(up, BDi[0]) + nn(up, BDi[1])
        Si[...] = nn(up, BDi[2]) + nn(up, BDi[3])
        fr, fi = prow[0:1, :], prow[1:2, :]
        pr, pi = pw[0, 0:1, :], pw[1, 0:1, :]
        sr = jnp.zeros((8, NST), F32)
        si = jnp.zeros((8, NST), F32)
        for i in range(16):
            at = slice(8 * i, 8 * i + 8)
            br, bi = cmul(fr, fi, Sr[at, :], Si[at, :])
            sr, si = cmul(pr, pi, sr, si)
            sr, si = sr + br, si + bi
            Sr[at, :] = sr
            Si[at, :] = si
        Er[...] = sr
        Ei[...] = si
        qr, qi = prow[2:3, :], prow[3:4, :]
        cr = jnp.zeros((1, NST), F32)
        ci = jnp.zeros((1, NST), F32)
        for j in range(8):
            cr, ci = cmul(qr, qi, cr, ci)
            cr, ci = cr + Er[j : j + 1, :], ci + Ei[j : j + 1, :]
        CY[y, 0:1, :] = cr
        CY[y, 1:2, :] = ci

        for j in range(1, RING):
            carry_copy(CY, cy_ss, cy_rs, y, (z * RING + ring(y, j), t)).start()

    def carry_row():
        carry_all(CY, cy_ss, cy_rs).wait_recv()
        br, bi = prow[4:5, :], prow[5:6, :]
        cr = jnp.zeros((1, NST), F32)
        ci = jnp.zeros((1, NST), F32)
        rowr, rowi = cr, ci
        wr, wi = cr + 1.0, ci
        for j in range(RING):
            keep = jnp.where(y == j, 1.0, 0.0).astype(F32)
            rowr = rowr + keep * cr
            rowi = rowi + keep * ci
            cr, ci = cmul(br, bi, cr, ci)
            cr, ci = cr + CY[j, 0:1, :], ci + CY[j, 1:2, :]
            go = jnp.where(y > j, 1.0, 0.0).astype(F32)
            nr, ni = cmul(br, bi, wr, wi)
            wr = wr + go * (nr - wr)
            wi = wi + go * (ni - wi)
        CZ[z, 0:1, :] = cr
        CZ[z, 1:2, :] = ci
        Cr[0:1, :] = rowr
        Ci[0:1, :] = rowi
        Cr[1:2, :] = wr
        Ci[1:2, :] = wi
        for j in range(1, RING):
            carry_copy(CZ, cz_ss, cz_rs, z, (ring(z, j) * RING + y, t)).start()


    def carry_column():
        qr, qi = prow[2:3, :], prow[3:4, :]
        carry_all(CZ, cz_ss, cz_rs).wait_recv()
        br, bi = prow[6:7, :], prow[7:8, :]
        cr = jnp.zeros((1, NST), F32)
        ci = jnp.zeros((1, NST), F32)
        for j in range(RING - 1):
            go = jnp.where(z > j, 1.0, 0.0).astype(F32)
            nr, ni = cmul(br, bi, cr, ci)
            nr, ni = nr + CZ[j, 0:1, :], ni + CZ[j, 1:2, :]
            cr = go * nr + (1.0 - go) * cr
            ci = go * ni + (1.0 - go) * ci
        cr, ci = cmul(Cr[1:2, :], Ci[1:2, :], cr, ci)
        cr, ci = cr + Cr[0:1, :], ci + Ci[0:1, :]
        for j in range(8):
            Cr[j : j + 1, :] = cr
            Ci[j : j + 1, :] = ci
            cr, ci = cmul(qr, qi, cr, ci)
            cr, ci = cr + Er[j : j + 1, :], ci + Ei[j : j + 1, :]
        cr, ci = Cr[...], Ci[...]
        for i in range(16):
            at = slice(8 * i, 8 * i + 8)
            gr, gi = cmul(pw[0, i : i + 1, :], pw[1, i : i + 1, :], cr, ci)
            Sr[at, :] = Sr[at, :] + gr
            Si[at, :] = Si[at, :] + gi
        total = upr[...].astype(F32) * sg[...]
        for j, ref in ((0, Sr), (2, Si)):
            high, low = split(ref[...])
            total = total + nt(high, BDo[j]) + nt(low, BDo[j])
        mixed = jax.nn.gelu(total).astype(BF16)
        M[:, 256:512] = lax.dot_general(
            permute, mixed, (((0,), (0,)), ((), ())), preferred_element_type=F32
        ).astype(BF16)


    def keys():
        kv = qkv[:, 256:384]
        key_lane = lane_full < 64
        kv = kv * jnp.where(key_lane, cosr[...], 1.0) + swapped(kv) * jnp.where(
            key_lane, sinr[...], 0.0
        )
        KVb[1] = kv.astype(BF16)
        kv_copy.start()

        for pair in range(2):
            x = qkv[:, 128 * pair : 128 * pair + 128]
            qb[:, 128 * pair : 128 * pair + 128] = (x * cosr[...] + swapped(x) * sinr[...]).astype(BF16)

    def attention():
        kv_copy.wait_recv()
        both = KVb[...].reshape(2 * ROWS, 128).astype(F32)
        turned = pltpu.roll(both, 64, 1)
        first_half = iota((2 * ROWS, 128), 1) < 64
        k_low = jnp.where(first_half, both, 0.0).astype(BF16)
        k_high = jnp.where(first_half, 0.0, turned).astype(BF16)
        v_low = jnp.where(first_half, turned, 0.0).astype(BF16)
        v_high = jnp.where(first_half, 0.0, both).astype(BF16)
        gap = iota((ROWS, 2 * ROWS), 0) + ROWS - iota((ROWS, 2 * ROWS), 1)
        key_at = sp * ROWS - ROWS + iota((ROWS, 2 * ROWS), 1)
        visible = (gap >= 0) & (gap < ROWS) & (key_at >= 0)

        def attend(pair):
            q = qb[:, 128 * pair : 128 * pair + 128]
            total = None
            for side, (k, v) in enumerate(((k_low, v_low), (k_high, v_high))):
                score = jnp.where(visible, nt(q, k) * 0.125, -jnp.inf)
                sink = sink_s[2 * pair + side]
                top = jnp.maximum(jnp.max(score, axis=-1, keepdims=True), sink)
                e = jnp.exp(score - top)
                weight = e / (jnp.sum(e, axis=-1, keepdims=True) + jnp.exp(sink - top))
                part = nn(weight.astype(BF16), v)
                total = part if total is None else total + part
            M[:, 128 * pair : 128 * pair + 128] = total.astype(BF16)


        attend(0)
        attend(1)

    def chunk(half, a, slot=None):
        wide = Wo[half, pl.ds(pl.multiple_of(a * RING, RING), RING)].reshape(256, 512)
        part = nt(M[...], wide)
        at = a + RING * half
        if slot is not None:
            Pl[slot] = part.astype(BF16).reshape(TP, 16, 256)
            Rl[t, slot] = Pl[slot, t]
            return at
        part = part.reshape(CHIPS, 2, 16, 256)
        PP[0, at] = part[:, 0]
        PP[1, at] = part[:, 1]
        return at

    def make(batch, items):
        made = [chunk(half, a) for half, a in items]
        for at in made:
            pltpu.make_async_remote_copy(
                src_ref=PP.at[1 - core, at], dst_ref=PR.at[at], send_sem=tw_ss,
                recv_sem=tw_rs.at[batch], device_id=twin, device_id_type=MESH,
            ).start()
        return made

    def twin_all(batch, count):
        ref = PR.at[pl.ds(0, count)]
        return pltpu.make_async_remote_copy(
            src_ref=ref, dst_ref=ref, send_sem=tw_ss, recv_sem=tw_rs.at[batch],
            device_id=twin, device_id_type=MESH,
        )

    def pass_on(batch, made):
        twin_all(batch, len(made)).wait_recv()
        for at in made:
            Pb[at] = (PP[core, at] + PR[at]).astype(BF16)
            R[chip, at] = Pb[at, chip]
        for at in made:
            for j in (2, 1, 3):
                to = lax.rem(chip + j, CHIPS)
                pltpu.make_async_remote_copy(
                    src_ref=Pb.at[at, to], dst_ref=R.at[chip, at], send_sem=rs_ss,
                    recv_sem=rs_rs.at[batch], device_id=(sp, 2 * to + core), device_id_type=MESH,
                ).start()

    def owned_all(batch, count):
        ref = R.at[pl.ds(0, CHIPS - 1), pl.ds(0, count)]
        return pltpu.make_async_remote_copy(
            src_ref=ref, dst_ref=ref, send_sem=rs_ss, recv_sem=rs_rs.at[batch],
            device_id=twin, device_id_type=MESH,
        )

    def add_up(batch, made):
        owned_all(batch, len(made)).wait_recv()
        for at in made:
            total = R[0, at].astype(F32)
            for j in range(1, CHIPS):
                total = total + R[j, at].astype(F32)
            T[at] = total

    def make_last():
        made = []
        for slot, (half, a) in enumerate(at_hop(4)):
            made.append(chunk(half, a, slot))
            for j in (4, 5, 2, 3, 6, 7, 1):
                to = 2 * lax.rem(chip + j // 2, CHIPS) + lax.rem(core + j, 2)
                pltpu.make_async_remote_copy(
                    src_ref=Pl.at[slot, to], dst_ref=Rl.at[t, slot], send_sem=last_ss,
                    recv_sem=last_rs, device_id=(sp, to), device_id_type=MESH,
                ).start()
        return made

    def last_all():
        ref = Rl.at[pl.ds(0, TP - 1)]
        return pltpu.make_async_remote_copy(
            src_ref=ref, dst_ref=ref, send_sem=last_ss, recv_sem=last_rs,
            device_id=twin, device_id_type=MESH,
        )

    gathers = {"S": wst, "Q": wqk, "O": wout}
    outs = {"S": (Ws, us), "Q": (Wq, qkv)}
    calls = {
        "norm": norm, "halves": halves, "tables": tables, "params": params, "in": diag_in,
        "out": diag_out, "scan": scan, "row": carry_row, "column": carry_column, "keys": keys,
        "attention": attention,
    }
    made = {}
    for name, *where in ORDER:
        if name == "stage":
            gathers[where[0]].stage(where[1])
        elif name == "forward":
            gathers[where[0]].forward(where[1], where[2])
        elif name == "project":
            if where[1] == 4:
                gathers[where[0]].last()
            projects(*outs[where[0]], where[1])
        elif name == "make":
            batch = where[0]
            made[batch] = make(batch, at_hop(0) + at_hop(1) if batch == 0 else at_hop(batch + 1))
        elif name == "pass_on":
            pass_on(where[0], made[where[0]])
        else:
            calls[name]()
    wout.last()
    made3 = make_last()
    for batch in range(3):
        add_up(batch, made[batch])

    twin_all(0, 14).wait_send()
    kv_copy.wait_send()
    carry_all(CY, cy_ss, cy_rs).wait_send()
    carry_all(CZ, cz_ss, cz_rs).wait_send()
    wst.drain()
    wqk.drain()
    wout.drain()
    owned_all(0, 14).wait_send()
    last_all().wait_send()
    last_all().wait_recv()
    for slot, at in enumerate(made3):
        total = Rl[0, slot].astype(F32)
        for j in range(1, TP):
            total = total + Rl[j, slot].astype(F32)
        T[at] = total

    def total_square():
        square = jnp.zeros((16, 256), F32)
        for at in range(2 * RING):
            square = square + T[at] * T[at]
        return jnp.sum(square, axis=-1, keepdims=True)

    square = total_square()
    scale = lax.rsqrt(square * (1.0 / D) + EPS)
    quarter = iota((16, 128), 1) // 32
    for n in range(32):
        zz, y0 = n // 4, 2 * (n % 4)
        tile = None
        pieces = ((y0, zz), (RING + zz, y0), (y0 + 1, zz), (RING + zz, y0 + 1))
        for place, (source, at) in enumerate(pieces):
            part = T[source, :, 128 * (at // 4) : 128 * (at // 4) + 128]
            shift = (32 * place - 32 * (at % 4)) % 128
            if shift:
                part = pltpu.roll(part, shift, 1)
            tile = part if tile is None else jnp.where(quarter == place, part, tile)
        cols = slice(128 * n, 128 * n + 128)
        out_ref[:, cols] = (tile * scale * og[:, cols]).astype(BF16)


def body(
    tokens, norm_gain, w_query, w_key, w_value, w_state_in, sink_logit, decay_rate, rotation,
    log_step, in_re, in_im, out_re, out_im, skip_gain, w_attn_out, w_state_out, out_gain,
):
    vm, dma = pltpu.VMEM, pltpu.SemaphoreType.DMA
    spec = pl.BlockSpec(memory_space=pl.ANY)
    specs = [spec] * 18
    specs[6] = specs[9] = pl.BlockSpec(memory_space=pltpu.SMEM)
    return pl.pallas_call(
        kernel,
        out_shape=pltpu.VMEM((16, D), BF16),
        in_specs=specs,
        out_specs=pl.BlockSpec(memory_space=pltpu.VMEM),
        scratch_shapes=[
            vm((2, 64, 32, 256), BF16),
            vm((2, 64, 32, NQ), BF16),
            vm((2, 64, 32, 512), BF16),
            vm((ROWS, D), BF16),
            vm((ROWS, D), BF16),
            vm((2, RING, ROWS, 256), BF16),
            vm((64, 64), BF16),
            vm((64, 64), BF16),
            vm((1, D), F32),
            vm((1, D), F32),
            vm((1, 256), F32),
            vm((16, 64), F32),
            vm((16, 64), F32),
            vm((16, 16, 64), F32),
            vm((16, 16, 64), F32),
            vm((16, 16, 64), F32),
            vm((16, 16, 64), F32),
            vm((ROWS, 256), F32),
            vm((ROWS, NQ), F32),
            vm((ROWS, 128), F32),
            vm((ROWS, 128), F32),
            vm((8, NST), F32),
            vm((2, 16, NST), F32),
            vm((4, 256, NST), BF16),
            vm((4, 256, NST), BF16),
            vm((ROWS, NST), F32),
            vm((ROWS, NST), F32),
            vm((8, NST), F32),
            vm((8, NST), F32),
            vm((8, NST), F32),
            vm((8, NST), F32),
            vm((RING, 2, NST), F32),
            vm((RING, 2, NST), F32),
            vm((2, ROWS, 128), BF16),
            vm((ROWS, 256), BF16),
            vm((ROWS, 512), BF16),
            vm((2, 2 * RING, CHIPS, 16, 256), F32),
            vm((2 * RING, CHIPS, 16, 256), F32),
            vm((2 * RING, CHIPS, 16, 256), BF16),
            vm((CHIPS, 2 * RING, 16, 256), BF16),
            vm((2, TP, 16, 256), BF16),
            vm((TP, 2, 16, 256), BF16),
            vm((2 * RING, 16, 256), F32),
            vm((ROWS, 256), BF16),
            dma((20,)),
            dma, dma((4,)), dma((16,)),
            dma, dma((4,)), dma((16,)),
            dma, dma((4,)), dma((16,)),
            dma, dma, dma, dma, dma, dma, dma, dma((3,)), dma, dma((3,)), dma, dma,
        ],
        compiler_params=pltpu.CompilerParams(collective_id=0, has_side_effects=True),
    )(
        tokens, norm_gain.reshape(1, D), w_query, w_key, w_value, w_state_in, sink_logit,
        decay_rate, rotation, log_step, in_re.transpose(0, 2, 1), in_im.transpose(0, 2, 1),
        out_re, out_im, skip_gain.reshape(1, 256), w_attn_out.T, w_state_out.T, out_gain.reshape(1, D),
    )


def solution(mesh):
    return jax.shard_map(
        body,
        mesh=mesh,
        in_specs=(
            P("sp", None),
            P(),
            P("sp", "tp"),
            P("sp", "tp"),
            P("sp", "tp"),
            P("sp", "tp"),
            P("tp"),
            P("tp", None),
            P("tp", None),
            P("tp"),
            P("tp", None, None),
            P("tp", None, None),
            P("tp", None, None),
            P("tp", None, None),
            P("tp"),
            P("tp", "sp"),
            P("tp", "sp"),
            P(),
        ),
        out_specs=P(("sp", "tp"), None),
        check_vma=False,
    )
```
